128 devices in a mesh: sp: 64 (over z, y, x), tp: 2 (over core).
Axes of the slice: x: 4, y: 4, z: 4, core: 2. Of those that a mesh axis runs over, the one named last changes fastest.
Arguments:
- tokens: bfloat16 [32768, 4096], P(('sp', 'tp')), may hold values from -6 to 6
- norm_gain: float32 [4096], replicated, may hold values from 0.5 to 1.5
- query_weight: bfloat16 [4096, 1024], P(None, 'tp'), may hold values from -0.09375 to 0.09375
- key_weight: bfloat16 [4096, 1024], P(None, 'tp'), may hold values from -0.09375 to 0.09375
- value_weight: bfloat16 [4096, 2048], P(None, 'tp'), may hold values from -0.09375 to 0.09375
- gate_weight: bfloat16 [4096, 2048], P(None, 'tp'), may hold values from -0.09375 to 0.09375
- decay_bias: float32 [1024], P('tp'), may hold values from -0.5 to 0.5
- head_gain: float32 [2048], P('tp'), may hold values from 0.5 to 1.5
- out_weight: bfloat16 [2048, 4096], P('tp'), may hold values from -0.125 to 0.125
Outputs:
- layer_out: bfloat16 [32768, 4096], P(('sp', 'tp'))
The draws below stay inside these ranges and needn't reach their ends.
All inputs are finite; a program needn't handle non-finite values.
Results may differ from the reference program's by a relative error of at most 0.015.
Values may be sent and summed in bfloat16 or wider, within the bound.
No kernel may reach another device: no remote copies, remote signals or barrier semaphores. Data moves between devices by JAX's collectives and lax.ppermute only.
A program may use at most 192 MiB of HBM per device.

```python
import math
import jax
import jax.numpy as jnp
from jax import lax

D = 4096
HEADS = 8
HEAD_K = 128
HEAD_V = 256
BLOCK = 64
SEQ = 32768
KEY_DIM = 1024
VALUE_DIM = 2048


def level_of(own_key, dims, cuts, least, top_value):
    level, own = 1.0, jax.random.fold_in(own_key, 6)
    for axis_at, shards_of in cuts:
        steps = jnp.exp(jax.random.uniform(jax.random.fold_in(own, axis_at), (shards_of,), jnp.float32, least / len(cuts), top_value / len(cuts)))
        level = level * jnp.repeat(steps, dims[axis_at] // shards_of).reshape([-1 if axis == axis_at else 1 for axis in range(len(dims))])
    return level


def bell_draw(rng, extent, spread, reach, shards=(), kind=jnp.bfloat16):
    gain = level_of(rng, extent, shards, -0.22, 0.18) if shards else 1.0
    array = jax.random.normal(rng, extent, jnp.float32) * spread * gain
    return jnp.minimum(jnp.maximum(array, -reach), reach).astype(kind)


def setup_inputs(seed: int = 0) -> dict:
    key_list = jax.random.split(jax.random.key(seed), 10)
    tokens = bell_draw(key_list[0], (SEQ, D), 1.0, 6.0, ((0, 128),))
    norm_gain = jnp.clip(1.0 + 0.1 * jax.random.normal(key_list[1], (D,), jnp.float32), 0.5, 1.5)
    query_weight = bell_draw(key_list[2], (D, KEY_DIM), D ** -0.5, 0.09375, ((1, 2),))
    key_weight = bell_draw(key_list[3], (D, KEY_DIM), D ** -0.5, 0.09375, ((1, 2),))
    value_weight = bell_draw(key_list[4], (D, VALUE_DIM), D ** -0.5, 0.09375, ((1, 2),))
    gate_weight = bell_draw(key_list[5], (D, VALUE_DIM), D ** -0.5, 0.09375, ((1, 2),))
    decay_bias = jnp.clip(jax.random.uniform(key_list[6], (KEY_DIM,), jnp.float32, -0.5, 0.5) * level_of(key_list[6], (KEY_DIM,), ((0, 2),), -0.4, 0.0), -0.5, 0.5)
    head_gain = jnp.clip(1.0 + 0.1 * jax.random.normal(key_list[7], (VALUE_DIM,), jnp.float32), 0.5, 1.5)
    out_weight = bell_draw(key_list[8], (VALUE_DIM, D), VALUE_DIM ** -0.5, 0.125, ((0, 2),))
    return {"tokens": tokens, "norm_gain": norm_gain, "query_weight": query_weight, "key_weight": key_weight, "value_weight": value_weight, "gate_weight": gate_weight, "decay_bias": decay_bias, "head_gain": head_gain, "out_weight": out_weight}


epsilon = 1e-06
decay_power = 16.0
precise = lax.Precision.HIGHEST

def to_blocks(values, head_count, head_width):
    block_count = values.shape[0] // BLOCK
    return values.astype(jnp.float32).reshape(block_count, BLOCK, head_count, head_width).transpose(0, 2, 1, 3)

def reference(tokens, norm_gain, query_weight, key_weight, value_weight, gate_weight, decay_bias, head_gain, out_weight):
    inputs = tokens.astype(jnp.float32)
    row_scale = lax.rsqrt(lax.optimization_barrier(jnp.mean(inputs * inputs, axis=-1, keepdims=True)) + epsilon)
    normed = (inputs * row_scale * norm_gain.astype(jnp.float32)).astype(jnp.bfloat16)
    query_rows = jnp.dot(normed, query_weight, preferred_element_type=jnp.float32).astype(jnp.bfloat16)
    key_rows = jnp.dot(normed, key_weight, preferred_element_type=jnp.float32).astype(jnp.bfloat16)
    value_rows = jnp.dot(normed, value_weight, preferred_element_type=jnp.float32).astype(jnp.bfloat16)
    gate_input = jnp.dot(normed, gate_weight, preferred_element_type=jnp.float32).astype(jnp.bfloat16)
    logits = decay_bias.astype(jnp.float32) + math.log(SEQ / 8.0)
    log_decay = jnp.broadcast_to(jax.nn.log_sigmoid(logits) / decay_power, (SEQ, KEY_DIM))
    query_blocks = to_blocks(query_rows, HEADS, HEAD_K) * HEAD_K ** (-0.5)
    key_blocks = to_blocks(key_rows, HEADS, HEAD_K)
    value_blocks = to_blocks(value_rows, HEADS, HEAD_V)
    decay_blocks = to_blocks(log_decay, HEADS, HEAD_K)
    within = jnp.cumsum(decay_blocks, axis=2)
    block_end = within[:, :, -1:, :]
    query_in = query_blocks * jnp.exp(within)
    key_in = key_blocks * jnp.exp(-within)
    key_out = key_blocks * jnp.exp(block_end - within)
    causal = jnp.tril(jnp.ones((BLOCK, BLOCK), dtype=bool))
    scores = jnp.where(causal, jnp.einsum('nhid,nhjd->nhij', query_in, key_in, precision=precise), 0.0)
    local_out = jnp.einsum('nhij,nhjv->nhiv', scores, value_blocks, precision=precise)
    block_decay = jnp.exp(block_end[:, :, 0, :])

    def advance(carry_state, inputs_now):
        query_now, key_now, value_now, decay_now = inputs_now
        carried = jnp.einsum('hid,hdv->hiv', query_now, carry_state, precision=precise)
        carry_state = decay_now[..., None] * carry_state + jnp.einsum('hjd,hjv->hdv', key_now, value_now, precision=precise)
        return (carry_state, carried)
    start_state = jnp.zeros((HEADS, HEAD_K, HEAD_V), jnp.float32)
    _, carried_out = lax.scan(advance, start_state, (query_in, key_out, value_blocks, block_decay))
    mixed_heads = (local_out + carried_out).transpose(0, 2, 1, 3).reshape(SEQ, HEADS, HEAD_V)
    head_scale = lax.rsqrt(lax.optimization_barrier(jnp.mean(mixed_heads * mixed_heads, axis=-1, keepdims=True)) + epsilon)
    normed_heads = (mixed_heads * head_scale * head_gain.astype(jnp.float32).reshape(HEADS, HEAD_V)).reshape(SEQ, HEADS * HEAD_V)
    gated_rows = (normed_heads * jax.nn.silu(gate_input.astype(jnp.float32))).astype(jnp.bfloat16)
    return jnp.dot(gated_rows, out_weight, preferred_element_type=jnp.float32).astype(jnp.bfloat16)
```

```python
import functools
import math

import jax
import jax.numpy as jnp
from jax import lax
from jax.experimental import pallas as pl
from jax.experimental.pallas import tpu as pltpu
from jax.sharding import Mesh
from jax.sharding import PartitionSpec as P

HEAD_K = 128
HEAD_V = 256
AXES = ("z", "y1", "y0", "x", "tp")
SP = ("z", "y1", "y0", "x")
INNER = ("y1", "y0", "x")
OUTER = ("z",)
EPS = 1e-06
VMEM_LIMIT = 58 * 1024 * 1024
COLS = 256


def vmem(shape=None):
    return pl.BlockSpec(memory_space=pltpu.VMEM)


def hbm():
    return pl.BlockSpec(memory_space=pl.ANY)


def params(**more):
    return pltpu.CompilerParams(vmem_limit_bytes=VMEM_LIMIT, **more)


def kv_body(at_ref, x_hbm, gain_ref, ld_ref, wk_hbm, wv_hbm, *rest, second):
    if second:
        prev_ref = rest[0]
        rest = rest[4:]
    xn_hbm, k_hbm, v_hbm, s_ref, x_buf, xn_buf, wk_buf, wv_buf, k_buf, v_buf, sems, out_sems = rest
    rows, depth = x_buf.shape
    key_width, value_width = k_buf.shape[1], v_buf.shape[1]
    half = at_ref[1]
    copies = []
    in_x = pltpu.make_async_copy(x_hbm, x_buf, sems.at[0])
    in_x.start()
    for j in range(key_width // COLS):
        cut = pl.ds(j * COLS, COLS)
        copies.append(pltpu.make_async_copy(wk_hbm.at[:, cut], wk_buf.at[j], sems.at[1 + j]))
    key_steps = len(copies)
    for j in range(value_width // COLS):
        cut = pl.ds(j * COLS, COLS)
        copies.append(
            pltpu.make_async_copy(wv_hbm.at[:, cut], wv_buf.at[j], sems.at[1 + key_steps + j])
        )
    for copy in copies:
        copy.start()
    in_x.wait()
    step = 32

    def normalize(i, carry):
        cut = pl.ds(pl.multiple_of(i * step, step), step)
        x = x_buf[cut, :].astype(jnp.float32)
        scale = lax.rsqrt(jnp.mean(x * x, axis=-1, keepdims=True) + EPS)
        xn_buf[cut, :] = (x * scale * gain_ref[...]).astype(jnp.bfloat16)
        return carry

    lax.fori_loop(0, rows // step, normalize, 0)
    out_xn = pltpu.make_async_copy(xn_buf, xn_hbm.at[half], out_sems.at[0])
    out_xn.start()
    position = (at_ref[0] + 1 + lax.broadcasted_iota(jnp.int32, (rows, COLS), 0)).astype(jnp.float32)
    for j, copy in enumerate(copies):
        copy.wait()
        if j < key_steps:
            cut = slice(j * COLS, (j + 1) * COLS)
            acc = jnp.dot(xn_buf[...], wk_buf[j], preferred_element_type=jnp.float32)
            k_buf[:, cut] = (acc * jnp.exp(-ld_ref[:, cut] * position)).astype(jnp.bfloat16)
        else:
            i = j - key_steps
            acc = jnp.dot(xn_buf[...], wv_buf[i], preferred_element_type=jnp.float32)
            v_buf[:, i * COLS : (i + 1) * COLS] = acc.astype(jnp.bfloat16)
    out_k = pltpu.make_async_copy(k_buf, k_hbm.at[half], out_sems.at[1])
    out_v = pltpu.make_async_copy(v_buf, v_hbm.at[half], out_sems.at[2])
    out_k.start()
    out_v.start()
    for h in range(key_width // HEAD_K):
        state = lax.dot_general(
            k_buf[:, h * HEAD_K : (h + 1) * HEAD_K],
            v_buf[:, h * HEAD_V : (h + 1) * HEAD_V],
            (((0,), (0,)), ((), ())),
            preferred_element_type=jnp.float32,
        )
        if second:
            state = state + prev_ref[h]
        s_ref[h] = state.astype(s_ref.dtype)
    out_xn.wait()
    out_k.wait()
    out_v.wait()


def project_kv(at, x, gain, ld, wk, wv, before=None):
    rows, depth = x.shape
    kw, vw = wk.shape[1], wv.shape[1]
    heads = kw // HEAD_K
    second = before is not None
    bf = jnp.bfloat16
    shapes = (
        jax.ShapeDtypeStruct((2, rows, depth), bf),
        jax.ShapeDtypeStruct((2, rows, kw), bf),
        jax.ShapeDtypeStruct((2, rows, vw), bf),
        jax.ShapeDtypeStruct((heads, HEAD_K, HEAD_V), bf if second else jnp.float32),
    )
    in_specs = [pl.BlockSpec(memory_space=pltpu.SMEM), hbm(), vmem(), vmem(), hbm(), hbm()]
    args = [at, x, gain, ld, wk, wv]
    aliases = {}
    if second:
        in_specs += [vmem(), hbm(), hbm(), hbm()]
        args += [before[3], before[0], before[1], before[2]]
        aliases = {7: 0, 8: 1, 9: 2}
    return pl.pallas_call(
        functools.partial(kv_body, second=second),
        out_shape=shapes,
        in_specs=in_specs,
        out_specs=(hbm(), hbm(), hbm(), vmem()),
        scratch_shapes=[
            pltpu.VMEM((rows, depth), bf),
            pltpu.VMEM((rows, depth), bf),
            pltpu.VMEM((kw // COLS, depth, COLS), bf),
            pltpu.VMEM((vw // COLS, depth, COLS), bf),
            pltpu.VMEM((rows, kw), bf),
            pltpu.VMEM((rows, vw), bf),
            pltpu.SemaphoreType.DMA((1 + (kw + vw) // COLS,)),
            pltpu.SemaphoreType.DMA((3,)),
        ],
        input_output_aliases=aliases,
        compiler_params=params(),
        name="kv_second" if second else "kv_first",
    )(*args)


def q_body(at_ref, xn_ref, w_ref, ld_ref, q_ref):
    rows = xn_ref.shape[0]
    position = (at_ref[0] + 1 + lax.broadcasted_iota(jnp.int32, (rows, COLS), 0)).astype(jnp.float32)
    acc = jnp.dot(xn_ref[...], w_ref[...], preferred_element_type=jnp.float32)
    q_ref[...] = (acc * (jnp.exp(ld_ref[...] * position) * HEAD_K ** (-0.5))).astype(jnp.bfloat16)


def g_body(xn_ref, w_ref, gain_ref, g_ref):
    acc = jnp.dot(xn_ref[...], w_ref[...], preferred_element_type=jnp.float32)
    g_ref[...] = (acc * gain_ref[...] / (1.0 + jnp.exp(-acc))).astype(jnp.bfloat16)


def project_q(at, xn, w, ld):
    rows, depth = xn.shape
    width = w.shape[1]
    return pl.pallas_call(
        q_body,
        out_shape=jax.ShapeDtypeStruct((rows, width), jnp.bfloat16),
        grid_spec=pltpu.PrefetchScalarGridSpec(
            num_scalar_prefetch=1,
            grid=(width // COLS,),
            in_specs=[
                pl.BlockSpec((rows, depth), lambda j, at: (0, 0), pipeline_mode=pl.Buffered(1)),
                pl.BlockSpec((depth, COLS), lambda j, at: (0, j)),
                pl.BlockSpec((1, COLS), lambda j, at: (0, j)),
            ],
            out_specs=pl.BlockSpec((rows, COLS), lambda j, at: (0, j)),
        ),
        compiler_params=params(),
        name="project_q",
    )(at, xn, w, ld)


def project_g(xn, w, gain):
    rows, depth = xn.shape
    width = w.shape[1]
    return pl.pallas_call(
        g_body,
        out_shape=jax.ShapeDtypeStruct((rows, width), jnp.bfloat16),
        grid=(width // COLS,),
        in_specs=[
            pl.BlockSpec((rows, depth), lambda j: (0, 0), pipeline_mode=pl.Buffered(1)),
            pl.BlockSpec((depth, COLS), lambda j: (0, j)),
            pl.BlockSpec((1, COLS), lambda j: (0, j)),
        ],
        out_specs=pl.BlockSpec((rows, COLS), lambda j: (0, j)),
        compiler_params=params(),
        name="project_g",
    )(xn, w, gain)


def local_body(q_ref, k_ref, v_ref, o_ref):
    rows = q_ref.shape[0]
    half = rows // 2
    f32 = jnp.float32
    nt = (((1,), (1,)), ((), ()))
    row = lax.broadcasted_iota(jnp.int32, (half, half), 0)
    col = lax.broadcasted_iota(jnp.int32, (half, half), 1)
    keep = row >= col
    for i in range(2):
        q = q_ref[i * half : (i + 1) * half, :]
        total = None
        for j in range(i + 1):
            part = slice(j * half, (j + 1) * half)
            scores = lax.dot_general(q, k_ref[part, :], nt, preferred_element_type=f32)
            if i == j:
                scores = jnp.where(keep, scores, 0.0)
            piece = jnp.dot(scores.astype(jnp.bfloat16), v_ref[part, :], preferred_element_type=f32)
            total = piece if total is None else total + piece
        o_ref[i * half : (i + 1) * half, :] = total


def attend_local(q, k, v):
    rows = q.shape[0]
    heads = q.shape[1] // HEAD_K
    return pl.pallas_call(
        local_body,
        out_shape=jax.ShapeDtypeStruct((rows, heads * HEAD_V), jnp.float32),
        grid=(heads,),
        in_specs=[
            pl.BlockSpec((rows, HEAD_K), lambda h: (0, h)),
            pl.BlockSpec((rows, HEAD_K), lambda h: (0, h)),
            pl.BlockSpec((rows, HEAD_V), lambda h: (0, h)),
        ],
        out_specs=pl.BlockSpec((rows, HEAD_V), lambda h: (0, h)),
        compiler_params=params(),
        name="attend_local",
    )(q, k, v)


def gate_rows(q, carried, local, gate):
    attended = local + jnp.dot(q, carried, preferred_element_type=jnp.float32)
    scale = lax.rsqrt(jnp.mean(attended * attended, axis=-1, keepdims=True) + EPS)
    return (attended * scale * gate.astype(jnp.float32)).astype(jnp.bfloat16)


def gate_body(at_ref, q_ref, s_ref, o_ref, g_ref, out_ref):
    out_ref[...] = gate_rows(q_ref[0], s_ref[0], o_ref[0], g_ref[0])


def gate_half(at, q, carried, local, gate):
    rows = q.shape[0] // 2
    heads = q.shape[1] // HEAD_K
    return pl.pallas_call(
        gate_body,
        out_shape=jax.ShapeDtypeStruct((rows, heads * HEAD_V), jnp.bfloat16),
        grid_spec=pltpu.PrefetchScalarGridSpec(
            num_scalar_prefetch=1,
            grid=(heads,),
            in_specs=[
                pl.BlockSpec((1, rows, HEAD_K), lambda h, at: (at[1], 0, h)),
                pl.BlockSpec((1, HEAD_K, HEAD_V), lambda h, at: (h, 0, 0)),
                pl.BlockSpec((1, rows, HEAD_V), lambda h, at: (at[1], 0, h)),
                pl.BlockSpec((1, rows, HEAD_V), lambda h, at: (at[1], 0, h)),
            ],
            out_specs=pl.BlockSpec((rows, HEAD_V), lambda h, at: (0, h)),
        ),
        compiler_params=params(),
        name="gate_half",
    )(at, q.reshape(2, rows, -1), carried, local.reshape(2, rows, -1), gate.reshape(2, rows, -1))


def out_own_body(a_ref, w_ref, o_ref):
    o_ref[...] = jnp.dot(a_ref[...], w_ref[...], preferred_element_type=jnp.float32)


def out_own(a, w):
    rows, depth = a.shape
    width = w.shape[1]
    cols = 512
    return pl.pallas_call(
        out_own_body,
        out_shape=jax.ShapeDtypeStruct((rows, width), jnp.float32),
        grid=(width // cols,),
        in_specs=[
            pl.BlockSpec((rows, depth), lambda j: (0, 0), pipeline_mode=pl.Buffered(1)),
            pl.BlockSpec((depth, cols), lambda j: (0, j)),
        ],
        out_specs=pl.BlockSpec((rows, cols), lambda j: (0, j)),
        compiler_params=params(),
        name="out_own",
    )(a, w)


def out_add_body(a_ref, w_ref, p_ref, o_ref):
    o_ref[...] = (
        p_ref[...] + jnp.dot(a_ref[...], w_ref[...], preferred_element_type=jnp.float32)
    ).astype(jnp.bfloat16)


def out_add(a, w, partial):
    rows, depth = a.shape
    width = w.shape[1]
    cols = 512
    return pl.pallas_call(
        out_add_body,
        out_shape=jax.ShapeDtypeStruct((rows, width), jnp.bfloat16),
        grid=(width // cols,),
        in_specs=[
            pl.BlockSpec((rows, depth), lambda j: (0, 0), pipeline_mode=pl.Buffered(1)),
            pl.BlockSpec((depth, cols), lambda j: (0, j)),
            pl.BlockSpec((rows, cols), lambda j: (0, j)),
        ],
        out_specs=pl.BlockSpec((rows, cols), lambda j: (0, j)),
        compiler_params=params(),
        name="out_add",
    )(a, w, partial)


def swap(x):
    return lax.ppermute(x, "tp", [(0, 1), (1, 0)])


def tied(*xs):
    return lax.optimization_barrier(xs)


def on_device(tokens, norm_gain, wq, wk, wv, wg, decay_bias, head_gain, wo):
    rows = tokens.shape[0]
    kw = wk.shape[1]
    heads = kw // HEAD_K
    tp = lax.axis_index("tp")
    stretch = lax.axis_index(SP)
    start = (stretch * (2 * rows)).astype(jnp.int32)
    sequence = lax.axis_size(SP) * 2 * rows
    logits = decay_bias.astype(jnp.float32) + math.log(sequence / 8.0)
    ld = (jax.nn.log_sigmoid(logits) / 16.0).reshape(1, kw)
    gain = norm_gain.astype(jnp.float32).reshape(1, -1)
    other_tokens = swap(tokens)

    def place(half):
        return jnp.stack([start + half * rows, half]).astype(jnp.int32)

    at_own, at_other = place(tp), place(1 - tp)
    first = project_kv(at_own, tokens, gain, ld, wk, wv)
    other_tokens, wo_send = tied(other_tokens, wo)
    other_wo = swap(wo_send)
    xn, k, v, state = project_kv(at_other, other_tokens, gain, ld, wk, wv, first)
    xn, k, v = (t.reshape(2 * rows, -1) for t in (xn, k, v))

    inner = lax.axis_size(INNER)
    pieces = state.reshape(inner, heads * HEAD_K // inner, HEAD_V)
    got = lax.all_to_all(pieces, INNER, 0, 0, tiled=True)
    q = project_q(place(0 * tp), xn, wq, ld)
    local = attend_local(q, k, v)
    got, local = tied(got, local)
    got = got.astype(jnp.float32)
    total = got.sum(0).astype(jnp.bfloat16)
    outer = lax.axis_size(OUTER)
    totals = lax.all_to_all(
        jnp.broadcast_to(total[None], (outer,) + total.shape), OUTER, 0, 0, tiled=True
    )
    xn, local = tied(xn, local)
    gate = project_g(xn, wg, head_gain.astype(jnp.float32).reshape(1, -1))
    totals, gate = tied(totals, gate)
    passed = (jnp.arange(outer) < lax.axis_index(OUTER))[:, None, None]
    far = jnp.where(passed, totals.astype(jnp.float32), 0.0).sum(0)
    run = far
    before = []
    for j in range(inner):
        before.append(run.astype(jnp.bfloat16))
        run = run + got[j]
    carried = lax.all_to_all(jnp.stack(before), INNER, 0, 0, tiled=True)
    carried = carried.reshape(heads, HEAD_K, HEAD_V)

    theirs = gate_half(at_other, q, carried, local, gate)
    received = swap(theirs)
    mine = gate_half(at_own, q, carried, local, gate)
    partial = out_own(mine, wo)
    return out_add(received, other_wo, partial)


def solution(mesh):
    z, y, x = 4, 4, 4
    finer = Mesh(mesh.devices.reshape(z, 2, 2, x, mesh.shape["tp"]), AXES)
    rows = P(AXES, None)
    cols = P(None, "tp")
    in_specs = (rows, P(), cols, cols, cols, cols, P("tp"), P("tp"), P("tp", None))
    return jax.shard_map(
        on_device, mesh=finer, in_specs=in_specs, out_specs=rows, check_vma=False
    )
```

```python
import functools
import math

import jax
import jax.numpy as jnp
from jax import lax
from jax.experimental import pallas as pl
from jax.experimental.pallas import tpu as pltpu
from jax.sharding import Mesh
from jax.sharding import PartitionSpec as P

HEAD_K = 128
HEAD_V = 256
AXES = ("z", "y", "x", "tp")
SP = ("z", "y", "x")
INNER = ("y", "x")
OUTER = "z"
EPS = 1e-06
COLS = 512
STEP = 64
MIB = 1024 * 1024
F32 = jnp.float32
BF16 = jnp.bfloat16
IN_VMEM = pl.BlockSpec(memory_space=pltpu.VMEM)
IN_HBM = pl.BlockSpec(memory_space=pl.ANY)
IN_SMEM = pl.BlockSpec(memory_space=pltpu.SMEM)


def call(body, outs, in_specs, args, scratch=(), limit=16, flops=0):
    size = sum(a.size * a.dtype.itemsize for a in args)
    kinds = {"vmem": (pltpu.VMEM, IN_VMEM), "hbm": (pltpu.HBM, IN_HBM)}
    out_shape = tuple(kinds[k][0](dims, dtype) for k, dims, dtype in outs)
    run = pl.pallas_call(
        body,
        out_shape=out_shape,
        in_specs=in_specs,
        out_specs=tuple(kinds[k][1] for k, _, _ in outs),
        scratch_shapes=scratch,
        compiler_params=pltpu.CompilerParams(vmem_limit_bytes=limit * MIB),
        cost_estimate=pl.CostEstimate(flops=flops, bytes_accessed=size, transcendentals=0),
    )
    out = run(*args)
    return out if len(out) > 1 else out[0]


def dot(a, b):
    return jnp.dot(a, b, preferred_element_type=F32)


def blocks(width, size=COLS):
    return [slice(c, c + size) for c in range(0, width, size)]


def column_copies(src, dst, sems, first):
    return [
        pltpu.make_async_copy(
            src.at[:, pl.ds(c, COLS)], dst.at[:, pl.ds(c, COLS)], sems.at[first + i]
        )
        for i, c in enumerate(range(0, src.shape[1], COLS))
    ]


def normalized(x, gain):
    x = x.astype(F32)
    scale = lax.rsqrt(jnp.mean(x * x, axis=-1, keepdims=True) + EPS)
    return (x * scale * gain).astype(BF16)


def log_decay(bias, sequence):
    logits = bias + math.log(sequence / 8.0)
    return -(jnp.maximum(-logits, 0.0) + jnp.log1p(jnp.exp(-jnp.abs(logits)))) / 16.0


def positions(start, rows):
    return (start + 1 + lax.broadcasted_iota(jnp.int32, (rows, COLS), 0)).astype(F32)


def put_keys(x, w, ld, position, k_ref, cut):
    k_ref[:, cut] = (dot(x, w) * jnp.exp(-ld[:, cut] * position)).astype(BF16)


def state_of(k_ref, v_ref, h):
    return lax.dot_general(
        k_ref[:, h * HEAD_K : (h + 1) * HEAD_K],
        v_ref[:, h * HEAD_V : (h + 1) * HEAD_V],
        (((0,), (0,)), ((), ())),
        preferred_element_type=F32,
    )


def send_out(k_ref, v_ref, k_hbm, v_hbm, sems):
    copies = [
        pltpu.make_async_copy(k_ref, k_hbm, sems.at[2]),
        pltpu.make_async_copy(v_ref, v_hbm, sems.at[3]),
    ]
    for copy in copies:
        copy.start()
    return copies


def first_body(
    start_ref, x_hbm, gain_hbm, bias_hbm, wk_hbm, wv_hbm, xn_hbm, wk_ref, wv_ref, k_hbm, v_hbm,
    s_ref, buf, xn_ref, k_ref, v_ref, gain_ref, bias_ref, sems, more_sems, *, sequence
):
    rows = buf.shape[0]
    small = [
        pltpu.make_async_copy(gain_hbm, gain_ref, more_sems.at[0]),
        pltpu.make_async_copy(bias_hbm, bias_ref, more_sems.at[1]),
    ]
    for copy in small:
        copy.start()
    in_x = [
        pltpu.make_async_copy(x_hbm.at[pl.ds(r, STEP), :], buf.at[pl.ds(r, STEP), :], sems.at[i])
        for i, r in enumerate(range(0, rows, STEP))
    ]
    in_k = column_copies(wk_hbm, wk_ref, sems, len(in_x))
    in_v = column_copies(wv_hbm, wv_ref, sems, len(in_x) + len(in_k))
    for copy in in_x + in_k + in_v:
        copy.start()
    for copy in small:
        copy.wait()
    ld = log_decay(bias_ref[...], sequence)
    for i, copy in enumerate(in_x):
        copy.wait()
        cut = slice(i * STEP, (i + 1) * STEP)
        xn_ref[cut, :] = normalized(buf[cut, :], gain_ref[...])
    out = pltpu.make_async_copy(xn_ref, xn_hbm, sems.at[len(in_x + in_k + in_v)])
    out.start()
    position = positions(start_ref[0], rows)
    for copy, cut in zip(in_k, blocks(wk_ref.shape[1])):
        copy.wait()
        put_keys(xn_ref[...], wk_ref[:, cut], ld, position, k_ref, cut)
    for copy, cut in zip(in_v, blocks(wv_ref.shape[1])):
        copy.wait()
        v_ref[:, cut] = dot(xn_ref[...], wv_ref[:, cut]).astype(BF16)
    out = [out] + send_out(k_ref, v_ref, k_hbm, v_hbm, more_sems)
    for h in range(s_ref.shape[0]):
        s_ref[h] = state_of(k_ref, v_ref, h)
    for copy in out:
        copy.wait()


def project_first(start, x, gain, bias, wk, wv, sequence):
    rows, depth = x.shape
    kw, vw = wk.shape[1], wv.shape[1]
    heads = kw // HEAD_K
    return call(
        functools.partial(first_body, sequence=sequence),
        [
            ("hbm", (rows, depth), BF16),
            ("vmem", (depth, kw), BF16),
            ("vmem", (depth, vw), BF16),
            ("hbm", (rows, kw), BF16),
            ("hbm", (rows, vw), BF16),
            ("vmem", (heads, HEAD_K, HEAD_V), F32),
        ],
        [IN_SMEM] + [IN_HBM] * 5,
        (start, x, gain, bias, wk, wv),
        scratch=[
            pltpu.VMEM((rows, depth), BF16),
            pltpu.VMEM((rows, depth), BF16),
            pltpu.VMEM((rows, kw), BF16),
            pltpu.VMEM((rows, vw), BF16),
            pltpu.VMEM(gain.shape, F32),
            pltpu.VMEM(bias.shape, F32),
            pltpu.SemaphoreType.DMA((rows // STEP + (kw + vw) // COLS + 1,)),
            pltpu.SemaphoreType.DMA((4,)),
        ],
        limit=24,
        flops=2 * rows * depth * (kw + vw),
    )


def second_body(
    start_ref, x_ref, gain_ref, bias_ref, wk_ref, wv_ref, prev_ref, xn_hbm, k_hbm, v_hbm, s_ref,
    sum_hbm, xn_ref, k_ref, v_ref, sum_buf, sems, more_sems, *, sequence
):
    rows = x_ref.shape[0]
    ld = log_decay(bias_ref[...], sequence)
    for cut in blocks(rows, STEP):
        xn_ref[cut, :] = normalized(x_ref[cut, :], gain_ref[...])
    out = [pltpu.make_async_copy(xn_ref, xn_hbm, sems.at[0])]
    out[0].start()
    position = positions(start_ref[0], rows)
    for cut in blocks(wk_ref.shape[1]):
        put_keys(xn_ref[...], wk_ref[:, cut], ld, position, k_ref, cut)
    for cut in blocks(wv_ref.shape[1]):
        v_ref[:, cut] = dot(xn_ref[...], wv_ref[:, cut]).astype(BF16)
    out += send_out(k_ref, v_ref, k_hbm, v_hbm, more_sems)
    for h in range(s_ref.shape[0]):
        state = state_of(k_ref, v_ref, h)
        s_ref[h] = state.astype(BF16)
        sum_buf[h] = (state + prev_ref[h]).astype(BF16)
        out.append(pltpu.make_async_copy(sum_buf.at[h], sum_hbm.at[h], sems.at[1 + h]))
        out[-1].start()
    for copy in out:
        copy.wait()


def project_second(start, x, gain, bias, wk, wv, before, sequence):
    rows, depth = x.shape
    kw, vw = wk.shape[1], wv.shape[1]
    heads = kw // HEAD_K
    return call(
        functools.partial(second_body, sequence=sequence),
        [
            ("hbm", (rows, depth), BF16),
            ("hbm", (rows, kw), BF16),
            ("hbm", (rows, vw), BF16),
            ("vmem", (heads, HEAD_K, HEAD_V), BF16),
            ("hbm", (heads, HEAD_K, HEAD_V), BF16),
        ],
        [IN_SMEM] + [IN_VMEM] * 6,
        (start, x, gain, bias, wk, wv, before),
        scratch=[
            pltpu.VMEM((rows, depth), BF16),
            pltpu.VMEM((rows, kw), BF16),
            pltpu.VMEM((rows, vw), BF16),
            pltpu.VMEM((heads, HEAD_K, HEAD_V), BF16),
            pltpu.SemaphoreType.DMA((1 + heads,)),
            pltpu.SemaphoreType.DMA((4,)),
        ],
        limit=24,
        flops=2 * rows * depth * (kw + vw),
    )


def query_body(
    tp_ref, at_ref, bt_ref, bias_ref, sa_ref, sb_ref, ka_hbm, kb_hbm, va_hbm, vb_hbm, xa_hbm,
    xb_hbm, w_hbm, qa_ref, qb_ref, oa_ref, ob_ref, xa_ref, xb_ref, w_ref, ka_ref, kb_ref, va_ref,
    vb_ref, sems, *, sequence
):
    copies = [
        pltpu.make_async_copy(src, dst, sems.at[i])
        for i, (src, dst) in enumerate(
            (
                (xa_hbm, xa_ref),
                (w_hbm, w_ref),
                (ka_hbm, ka_ref),
                (va_hbm, va_ref),
                (xb_hbm, xb_ref),
                (kb_hbm, kb_ref),
                (vb_hbm, vb_ref),
            )
        )
    ]
    for copy in copies:
        copy.start()
    upper = tp_ref[0].astype(F32)
    halves = (
        (at_ref, xa_ref, ka_ref, va_ref, qa_ref, oa_ref, sb_ref, upper, copies[:4]),
        (bt_ref, xb_ref, kb_ref, vb_ref, qb_ref, ob_ref, sa_ref, 1.0 - upper, copies[4:]),
    )
    rows = xa_ref.shape[0]
    ld = log_decay(bias_ref[...], sequence)
    keep = lax.broadcasted_iota(jnp.int32, (rows, rows), 0) >= lax.broadcasted_iota(
        jnp.int32, (rows, rows), 1
    )
    for start, x_ref, k_ref, v_ref, q_ref, o_ref, s_ref, later, needs in halves:
        for copy in needs:
            copy.wait()
        for cut in blocks(w_ref.shape[1]):
            decay = jnp.exp(ld[:, cut] * positions(start[0], rows)) * HEAD_K ** (-0.5)
            q_ref[:, cut] = (dot(x_ref[...], w_ref[:, cut]) * decay).astype(BF16)
        for h in range(w_ref.shape[1] // HEAD_K):
            key = slice(h * HEAD_K, (h + 1) * HEAD_K)
            value = slice(h * HEAD_V, (h + 1) * HEAD_V)
            scores = lax.dot_general(
                q_ref[:, key], k_ref[:, key], (((1,), (1,)), ((), ())), preferred_element_type=F32
            )
            scores = jnp.where(keep, scores, 0.0).astype(BF16)
            earlier = (s_ref[h].astype(F32) * later).astype(BF16)
            local = dot(scores, v_ref[:, value]) + dot(q_ref[:, key], earlier)
            o_ref[:, value] = local.astype(BF16)


def project_query(tp, at, bt, bias, sa, sb, ka, kb, va, vb, xa, xb, w, sequence):
    rows, depth = xa.shape
    kw, vw = w.shape[1], va.shape[1]
    return call(
        functools.partial(query_body, sequence=sequence),
        [
            ("vmem", (rows, kw), BF16),
            ("vmem", (rows, kw), BF16),
            ("vmem", (rows, vw), BF16),
            ("vmem", (rows, vw), BF16),
        ],
        [IN_SMEM] * 3 + [IN_VMEM] * 3 + [IN_HBM] * 7,
        (tp, at, bt, bias, sa, sb, ka, kb, va, vb, xa, xb, w),
        scratch=[
            pltpu.VMEM((rows, depth), BF16),
            pltpu.VMEM((rows, depth), BF16),
            pltpu.VMEM((depth, kw), BF16),
            pltpu.VMEM((rows, kw), BF16),
            pltpu.VMEM((rows, kw), BF16),
            pltpu.VMEM((rows, vw), BF16),
            pltpu.VMEM((rows, vw), BF16),
            pltpu.SemaphoreType.DMA((7,)),
        ],
        limit=32,
        flops=5 * rows * depth * kw,
    )


def gate_body(gain_ref, xa_hbm, xb_hbm, w_hbm, ga_ref, gb_ref, xa_ref, xb_ref, w_ref, sems):
    in_a = pltpu.make_async_copy(xa_hbm, xa_ref, sems.at[0])
    in_b = pltpu.make_async_copy(xb_hbm, xb_ref, sems.at[1])
    in_w = column_copies(w_hbm, w_ref, sems, 2)
    for copy in [in_a, in_w[0], in_b] + in_w[1:]:
        copy.start()
    in_a.wait()
    for i, (copy, cut) in enumerate(zip(in_w, blocks(w_ref.shape[1]))):
        copy.wait()
        for x_ref, g_ref in ((xa_ref, ga_ref), (xb_ref, gb_ref)):
            if i == 0 and x_ref is xb_ref:
                in_b.wait()
            acc = dot(x_ref[...], w_ref[:, cut])
            g_ref[:, cut] = (acc * gain_ref[:, cut] / (1.0 + jnp.exp(-acc))).astype(BF16)


def project_gate(gain, xa, xb, w):
    rows, depth = xa.shape
    width = w.shape[1]
    return call(
        gate_body,
        [("vmem", (rows, width), BF16), ("vmem", (rows, width), BF16)],
        [IN_VMEM] + [IN_HBM] * 3,
        (gain, xa, xb, w),
        scratch=[
            pltpu.VMEM((rows, depth), BF16),
            pltpu.VMEM((rows, depth), BF16),
            pltpu.VMEM((depth, width), BF16),
            pltpu.SemaphoreType.DMA((2 + width // COLS,)),
        ],
        limit=32,
        flops=4 * rows * depth * width,
    )


def total_body(got_ref, out_ref):
    total = got_ref[0].astype(F32)
    for j in range(1, got_ref.shape[0]):
        total = total + got_ref[j].astype(F32)
    for i in range(out_ref.shape[0]):
        out_ref[i] = total.astype(BF16)


def total_of(got, copies):
    outs = [("vmem", (copies,) + got.shape[1:], BF16)]
    return call(total_body, outs, [IN_VMEM], (got,), limit=4)


def before_body(at_ref, got_ref, totals_ref, out_ref):
    run = jnp.zeros(got_ref.shape[1:], F32)
    for i in range(totals_ref.shape[0]):
        run = run + jnp.where(i < at_ref[0], totals_ref[i].astype(F32), 0.0)
    for j in range(got_ref.shape[0]):
        out_ref[j] = run.astype(BF16)
        run = run + got_ref[j].astype(F32)


def before_of(at, got, totals):
    outs = [("vmem", got.shape, BF16)]
    specs = [IN_SMEM, IN_VMEM, IN_VMEM]
    return call(before_body, outs, specs, (at, got, totals), limit=4)


def gated(q_ref, c_ref, o_ref, g_ref, out_ref):
    for h in range(c_ref.shape[0]):
        key = slice(h * HEAD_K, (h + 1) * HEAD_K)
        value = slice(h * HEAD_V, (h + 1) * HEAD_V)
        attended = o_ref[:, value].astype(F32) + dot(q_ref[:, key], c_ref[h])
        scale = lax.rsqrt(jnp.mean(attended * attended, axis=-1, keepdims=True) + EPS)
        out_ref[:, value] = (attended * scale * g_ref[:, value].astype(F32)).astype(BF16)


def gate_theirs(q, c, o, g):
    outs = [("vmem", g.shape, BF16)]
    return call(gated, outs, [IN_VMEM] * 4, (q, c, o, g), limit=8, flops=10**9)


def mine_body(
    q_ref, c_ref, o_ref, g_ref, wa_hbm, wb_hbm, out_ref, wb_ref, wa_ref, rows_buf, sems
):
    in_a = column_copies(wa_hbm, wa_ref, sems, 0)
    in_b = column_copies(wb_hbm, wb_ref, sems, len(in_a))
    for copy in in_a + in_b:
        copy.start()
    gated(q_ref, c_ref, o_ref, g_ref, rows_buf)
    for copy, cut in zip(in_a, blocks(wa_ref.shape[1])):
        copy.wait()
        out_ref[:, cut] = dot(rows_buf[...], wa_ref[:, cut])
    for copy in in_b:
        copy.wait()


def out_mine(q, c, o, g, wa, wb):
    rows = q.shape[0]
    depth, width = wa.shape
    return call(
        mine_body,
        [("vmem", (rows, width), F32), ("vmem", (depth, width), BF16)],
        [IN_VMEM] * 4 + [IN_HBM] * 2,
        (q, c, o, g, wa, wb),
        scratch=[
            pltpu.VMEM((depth, width), BF16),
            pltpu.VMEM(g.shape, BF16),
            pltpu.SemaphoreType.DMA((2 * width // COLS,)),
        ],
        limit=32,
        flops=2 * rows * depth * width,
    )


def last_body(a_ref, w_ref, p_ref, out_hbm, buf, sems):
    copies = []
    for i, cut in enumerate(blocks(buf.shape[1])):
        buf[:, cut] = (p_ref[:, cut] + dot(a_ref[...], w_ref[:, cut])).astype(BF16)
        wide = pl.ds(i * COLS, COLS)
        copies.append(pltpu.make_async_copy(buf.at[:, wide], out_hbm.at[:, wide], sems.at[i]))
        copies[-1].start()
    for copy in copies:
        copy.wait()


def out_last(a, w, partial):
    rows, width = partial.shape
    return call(
        last_body,
        [("hbm", (rows, width), BF16)],
        [IN_VMEM] * 3,
        (a, w, partial),
        scratch=[pltpu.VMEM((rows, width), BF16), pltpu.SemaphoreType.DMA((width // COLS,))],
        limit=20,
        flops=2 * rows * w.shape[0] * width,
    )


def swap(x):
    return lax.ppermute(x, "tp", [(0, 1), (1, 0)])


def scalar(x):
    return x.astype(jnp.int32).reshape(1)


def mixer(tokens, norm_gain, wq, wk, wv, wg, decay_bias, head_gain, wo):
    rows = tokens.shape[0]
    kw = wk.shape[1]
    heads = kw // HEAD_K
    tp = lax.axis_index("tp").astype(jnp.int32)
    start = (lax.axis_index(SP) * (2 * rows)).astype(jnp.int32)
    at, bt = scalar(start + tp * rows), scalar(start + (1 - tp) * rows)
    sequence = lax.axis_size(SP) * 2 * rows
    bias = decay_bias.astype(F32).reshape(1, kw)
    gain = norm_gain.astype(F32).reshape(1, -1)
    out_gain = head_gain.astype(F32).reshape(1, -1)
    far = functools.partial(pltpu.with_memory_space_constraint, memory_space=pltpu.HBM)

    others = swap(tokens)
    other_wo = swap(wo)
    xa, wk, wv, ka, va, sa = project_first(
        at, *map(far, (tokens, gain, bias, wk, wv)), sequence
    )
    xb, kb, vb, sb, state = project_second(bt, others, gain, bias, wk, wv, sa, sequence)

    inner, outer = lax.axis_size(INNER), lax.axis_size(OUTER)
    pieces = state.reshape(inner, heads * HEAD_K // inner, HEAD_V)
    got = lax.all_to_all(pieces, INNER, 0, 0, tiled=True)
    qa, qb, oa, ob = project_query(
        scalar(tp), at, bt, bias, sa, sb, *map(far, (ka, kb, va, vb, xa, xb, wq)), sequence
    )
    totals = lax.all_to_all(total_of(got, outer), OUTER, 0, 0, tiled=True)
    before = before_of(scalar(lax.axis_index(OUTER)), got, totals)
    carried = lax.all_to_all(before, INNER, 0, 0, tiled=True)
    ga, gb = project_gate(out_gain, far(xa), far(xb), far(wg))
    carried = carried.reshape(heads, HEAD_K, HEAD_V)

    theirs = gate_theirs(qb, carried, ob, gb)
    received = swap(theirs)
    partial, wb = out_mine(qa, carried, oa, ga, far(wo), far(other_wo))
    return out_last(received, wb, partial)


def solution(mesh):
    z, y, x = 4, 4, 4
    finer = Mesh(mesh.devices.reshape(z, y, x, mesh.shape["tp"]), AXES)
    rows = P(AXES, None)
    cols = P(None, "tp")
    in_specs = (rows, P(), cols, cols, cols, cols, P("tp"), P("tp"), P("tp", None))
    return jax.shard_map(mixer, mesh=finer, in_specs=in_specs, out_specs=rows, check_vma=False)
```

```python
import functools
import math

import jax
import jax.numpy as jnp
from jax import lax
from jax.experimental import pallas as pl
from jax.experimental.pallas import tpu as pltpu
from jax.sharding import Mesh
from jax.sharding import PartitionSpec as P

HEAD_K = 128
HEAD_V = 256
AXES = ("z", "y", "x", "tp")
SP = ("z", "y", "x")
EPS = 1e-06
COLS = 512
STEP = 64
MIB = 1024 * 1024
F32 = jnp.float32
BF16 = jnp.bfloat16
IN_VMEM = pl.BlockSpec(memory_space=pltpu.VMEM)
IN_HBM = pl.BlockSpec(memory_space=pl.ANY)
IN_SMEM = pl.BlockSpec(memory_space=pltpu.SMEM)


def call(body, outs, in_specs, args, scratch=(), limit=16, flops=0):
    size = sum(a.size * a.dtype.itemsize for a in args)
    kinds = {"vmem": (pltpu.VMEM, IN_VMEM), "hbm": (pltpu.HBM, IN_HBM)}
    out_shape = tuple(kinds[k][0](dims, dtype) for k, dims, dtype in outs)
    run = pl.pallas_call(
        body,
        out_shape=out_shape,
        in_specs=in_specs,
        out_specs=tuple(kinds[k][1] for k, _, _ in outs),
        scratch_shapes=scratch,
        compiler_params=pltpu.CompilerParams(vmem_limit_bytes=limit * MIB),
        cost_estimate=pl.CostEstimate(flops=flops, bytes_accessed=size, transcendentals=0),
    )
    out = run(*args)
    return out if len(out) > 1 else out[0]


def dot(a, b):
    return jnp.dot(a, b, preferred_element_type=F32)


def blocks(width, size=COLS):
    return [slice(c, c + size) for c in range(0, width, size)]


def column_copies(src, dst, sems, first):
    return [
        pltpu.make_async_copy(
            src.at[:, pl.ds(c, COLS)], dst.at[:, pl.ds(c, COLS)], sems.at[first + i]
        )
        for i, c in enumerate(range(0, dst.shape[1], COLS))
    ]


def normalized(x, gain):
    x = x.astype(F32)
    scale = lax.rsqrt(jnp.mean(x * x, axis=-1, keepdims=True) + EPS)
    return (x * scale * gain).astype(BF16)


def log_decay(bias, sequence):
    logits = bias + math.log(sequence / 8.0)
    return -(jnp.maximum(-logits, 0.0) + jnp.log1p(jnp.exp(-jnp.abs(logits)))) / 16.0


def positions(start, rows):
    return (start + 1 + lax.broadcasted_iota(jnp.int32, (rows, COLS), 0)).astype(F32)


def put_keys(x, w, ld, position, k_ref, cut):
    k_ref[:, cut] = (dot(x, w) * jnp.exp(-ld[:, cut] * position)).astype(BF16)


def state_of(k_ref, v_ref, h):
    return lax.dot_general(
        k_ref[:, h * HEAD_K : (h + 1) * HEAD_K],
        v_ref[:, h * HEAD_V : (h + 1) * HEAD_V],
        (((0,), (0,)), ((), ())),
        preferred_element_type=F32,
    )


def first_body(
    start_ref, x_hbm, gain_hbm, bias_hbm, wk_hbm, wv_hbm, xn_ref, wk_ref, wv_ref, k_ref, v_ref,
    s_ref, buf, gain_ref, bias_ref, sems, *, sequence
):
    rows = buf.shape[0]
    small = [
        pltpu.make_async_copy(gain_hbm, gain_ref, sems.at[0]),
        pltpu.make_async_copy(bias_hbm, bias_ref, sems.at[1]),
    ]
    in_x = [
        pltpu.make_async_copy(
            x_hbm.at[pl.ds(r, STEP), :], buf.at[pl.ds(r, STEP), :], sems.at[2 + i]
        )
        for i, r in enumerate(range(0, rows, STEP))
    ]
    in_k = column_copies(wk_hbm, wk_ref, sems, 2 + len(in_x))
    in_v = column_copies(wv_hbm, wv_ref, sems, 2 + len(in_x) + len(in_k))
    for copy in small + in_x + in_k + in_v:
        copy.start()
    for copy in small:
        copy.wait()
    ld = log_decay(bias_ref[...], sequence)
    for i, copy in enumerate(in_x):
        copy.wait()
        cut = slice(i * STEP, (i + 1) * STEP)
        xn_ref[cut, :] = normalized(buf[cut, :], gain_ref[...])
    position = positions(start_ref[0], rows)
    for copy, cut in zip(in_k, blocks(wk_ref.shape[1])):
        copy.wait()
        put_keys(xn_ref[...], wk_ref[:, cut], ld, position, k_ref, cut)
    for copy, cut in zip(in_v, blocks(wv_ref.shape[1])):
        copy.wait()
        v_ref[:, cut] = dot(xn_ref[...], wv_ref[:, cut]).astype(BF16)
    for h in range(s_ref.shape[0]):
        s_ref[h] = state_of(k_ref, v_ref, h)


def project_first(start, x, gain, bias, wk, wv, sequence):
    rows, depth = x.shape
    kw, vw = wk.shape[1], wv.shape[1]
    heads = kw // HEAD_K
    return call(
        functools.partial(first_body, sequence=sequence),
        [
            ("vmem", (rows, depth), BF16),
            ("vmem", (depth, kw), BF16),
            ("vmem", (depth, vw), BF16),
            ("vmem", (rows, kw), BF16),
            ("vmem", (rows, vw), BF16),
            ("vmem", (heads, HEAD_K, HEAD_V), F32),
        ],
        [IN_SMEM] + [IN_HBM] * 5,
        (start, x, gain, bias, wk, wv),
        scratch=[
            pltpu.VMEM((rows, depth), BF16),
            pltpu.VMEM(gain.shape, F32),
            pltpu.VMEM(bias.shape, F32),
            pltpu.SemaphoreType.DMA((2 + rows // STEP + (kw + vw) // COLS,)),
        ],
        limit=24,
        flops=2 * rows * depth * (kw + vw),
    )


def second_body(
    start_ref, x_ref, gain_ref, bias_ref, wk_ref, wv_ref, prev_ref, xa_ref, ka_ref, va_ref,
    xa_hbm, ka_hbm, va_hbm, xn_hbm, k_hbm, v_hbm, s_hbm, sum_hbm, xn_ref, k_ref, v_ref, s_ref,
    sum_buf, sems, *, sequence
):
    rows = x_ref.shape[0]
    out = []

    def send(src, dst):
        out.append(pltpu.make_async_copy(src, dst, sems.at[len(out)]))
        out[-1].start()

    send(ka_ref, ka_hbm)
    send(va_ref, va_hbm)
    send(xa_ref, xa_hbm)
    ld = log_decay(bias_ref[...], sequence)
    for cut in blocks(rows, STEP):
        xn_ref[cut, :] = normalized(x_ref[cut, :], gain_ref[...])
    send(xn_ref, xn_hbm)
    position = positions(start_ref[0], rows)
    for cut in blocks(wk_ref.shape[1]):
        put_keys(xn_ref[...], wk_ref[:, cut], ld, position, k_ref, cut)
    for cut in blocks(wv_ref.shape[1]):
        v_ref[:, cut] = dot(xn_ref[...], wv_ref[:, cut]).astype(BF16)
    for h in range(s_ref.shape[0]):
        state = state_of(k_ref, v_ref, h)
        s_ref[h] = state.astype(BF16)
        sum_buf[h] = (state + prev_ref[h]).astype(BF16)
        send(sum_buf.at[h], sum_hbm.at[h])
    send(s_ref, s_hbm)
    send(k_ref, k_hbm)
    send(v_ref, v_hbm)
    for copy in out:
        copy.wait()


def project_second(start, x, gain, bias, wk, wv, before, xa, ka, va, sequence):
    rows, depth = x.shape
    kw, vw = wk.shape[1], wv.shape[1]
    heads = kw // HEAD_K
    half = [("hbm", (rows, depth), BF16), ("hbm", (rows, kw), BF16), ("hbm", (rows, vw), BF16)]
    return call(
        functools.partial(second_body, sequence=sequence),
        half
        + half
        + [("hbm", (heads, HEAD_K, HEAD_V), BF16)] * 2,
        [IN_SMEM] + [IN_VMEM] * 9,
        (start, x, gain, bias, wk, wv, before, xa, ka, va),
        scratch=[
            pltpu.VMEM((rows, depth), BF16),
            pltpu.VMEM((rows, kw), BF16),
            pltpu.VMEM((rows, vw), BF16),
            pltpu.VMEM((heads, HEAD_K, HEAD_V), BF16),
            pltpu.VMEM((heads, HEAD_K, HEAD_V), BF16),
            pltpu.SemaphoreType.DMA((7 + heads,)),
        ],
        limit=28,
        flops=2 * rows * depth * (kw + vw),
    )


def query_body(
    tp_ref, at_ref, bt_ref, bias_ref, sa_ref, sb_hbm, ka_hbm, kb_hbm, va_hbm, vb_hbm, xa_hbm,
    xb_hbm, w_hbm, qa_ref, qb_ref, oa_ref, ob_ref, xa_ref, xb_ref, w_ref, ka_ref, kb_ref, va_ref,
    vb_ref, sb_ref, sems, *, sequence
):
    copies = [
        pltpu.make_async_copy(src, dst, sems.at[i])
        for i, (src, dst) in enumerate(
            (
                (xa_hbm, xa_ref),
                (w_hbm, w_ref),
                (ka_hbm, ka_ref),
                (va_hbm, va_ref),
                (sb_hbm, sb_ref),
                (xb_hbm, xb_ref),
                (kb_hbm, kb_ref),
                (vb_hbm, vb_ref),
            )
        )
    ]
    for copy in copies:
        copy.start()
    upper = tp_ref[0].astype(F32)
    halves = (
        (at_ref, xa_ref, ka_ref, va_ref, qa_ref, oa_ref, sb_ref, upper, copies[:5]),
        (bt_ref, xb_ref, kb_ref, vb_ref, qb_ref, ob_ref, sa_ref, 1.0 - upper, copies[5:]),
    )
    rows = xa_ref.shape[0]
    ld = log_decay(bias_ref[...], sequence)
    keep = lax.broadcasted_iota(jnp.int32, (rows, rows), 0) >= lax.broadcasted_iota(
        jnp.int32, (rows, rows), 1
    )
    for start, x_ref, k_ref, v_ref, q_ref, o_ref, s_ref, later, needs in halves:
        for copy in needs:
            copy.wait()
        for cut in blocks(w_ref.shape[1]):
            decay = jnp.exp(ld[:, cut] * positions(start[0], rows)) * HEAD_K ** (-0.5)
            q_ref[:, cut] = (dot(x_ref[...], w_ref[:, cut]) * decay).astype(BF16)
        for h in range(w_ref.shape[1] // HEAD_K):
            key = slice(h * HEAD_K, (h + 1) * HEAD_K)
            value = slice(h * HEAD_V, (h + 1) * HEAD_V)
            scores = lax.dot_general(
                q_ref[:, key], k_ref[:, key], (((1,), (1,)), ((), ())), preferred_element_type=F32
            )
            scores = jnp.where(keep, scores, 0.0).astype(BF16)
            earlier = (s_ref[h].astype(F32) * later).astype(BF16)
            local = dot(scores, v_ref[:, value]) + dot(q_ref[:, key], earlier)
            o_ref[:, value] = local.astype(BF16)


def project_query(tp, at, bt, bias, sa, sb, ka, kb, va, vb, xa, xb, w, sequence):
    rows, depth = xa.shape
    kw, vw = w.shape[1], va.shape[1]
    return call(
        functools.partial(query_body, sequence=sequence),
        [
            ("vmem", (rows, kw), BF16),
            ("vmem", (rows, kw), BF16),
            ("vmem", (rows, vw), BF16),
            ("vmem", (rows, vw), BF16),
        ],
        [IN_SMEM] * 3 + [IN_VMEM] * 2 + [IN_HBM] * 8,
        (tp, at, bt, bias, sa, sb, ka, kb, va, vb, xa, xb, w),
        scratch=[
            pltpu.VMEM((rows, depth), BF16),
            pltpu.VMEM((rows, depth), BF16),
            pltpu.VMEM((depth, kw), BF16),
            pltpu.VMEM((rows, kw), BF16),
            pltpu.VMEM((rows, kw), BF16),
            pltpu.VMEM((rows, vw), BF16),
            pltpu.VMEM((rows, vw), BF16),
            pltpu.VMEM(sb.shape, BF16),
            pltpu.SemaphoreType.DMA((8,)),
        ],
        limit=32,
        flops=5 * rows * depth * kw,
    )


def gate_body(gain_ref, xa_hbm, xb_hbm, w_hbm, ga_ref, gb_ref, xa_ref, xb_ref, w_ref, sems):
    in_a = pltpu.make_async_copy(xa_hbm, xa_ref, sems.at[0])
    in_b = pltpu.make_async_copy(xb_hbm, xb_ref, sems.at[1])
    in_w = column_copies(w_hbm, w_ref, sems, 2)
    for copy in [in_a, in_w[0], in_b] + in_w[1:]:
        copy.start()
    in_a.wait()
    for i, (copy, cut) in enumerate(zip(in_w, blocks(w_ref.shape[1]))):
        copy.wait()
        for x_ref, g_ref in ((xa_ref, ga_ref), (xb_ref, gb_ref)):
            if i == 0 and x_ref is xb_ref:
                in_b.wait()
            acc = dot(x_ref[...], w_ref[:, cut])
            g_ref[:, cut] = (acc * gain_ref[:, cut] / (1.0 + jnp.exp(-acc))).astype(BF16)


def project_gate(gain, xa, xb, w):
    rows, depth = xa.shape
    width = w.shape[1]
    return call(
        gate_body,
        [("vmem", (rows, width), BF16), ("vmem", (rows, width), BF16)],
        [IN_VMEM] + [IN_HBM] * 3,
        (gain, xa, xb, w),
        scratch=[
            pltpu.VMEM((rows, depth), BF16),
            pltpu.VMEM((rows, depth), BF16),
            pltpu.VMEM((depth, width), BF16),
            pltpu.SemaphoreType.DMA((2 + width // COLS,)),
        ],
        limit=32,
        flops=4 * rows * depth * width,
    )


def before_body(got_ref, out_hbm, out_ref, sems):
    parts = sems.shape[0]
    count = got_ref.shape[0] // parts
    run = jnp.zeros(got_ref.shape[1:], F32)
    copies = []
    for i in range(parts):
        for j in range(i * count, (i + 1) * count):
            out_ref[j] = run.astype(BF16)
            run = run + got_ref[j].astype(F32)
        part = pl.ds(i * count, count)
        copies.append(pltpu.make_async_copy(out_ref.at[part], out_hbm.at[part], sems.at[i]))
        copies[-1].start()
    for copy in copies:
        copy.wait()


def before_of(got):
    return call(
        before_body,
        [("hbm", got.shape, BF16)],
        [IN_VMEM],
        (got,),
        scratch=[pltpu.VMEM(got.shape, BF16), pltpu.SemaphoreType.DMA((4,))],
        limit=4,
    )


def gated(q_ref, c_ref, o_ref, g_ref, out_ref):
    for h in range(c_ref.shape[0]):
        key = slice(h * HEAD_K, (h + 1) * HEAD_K)
        value = slice(h * HEAD_V, (h + 1) * HEAD_V)
        attended = o_ref[:, value].astype(F32) + dot(q_ref[:, key], c_ref[h])
        scale = lax.rsqrt(jnp.mean(attended * attended, axis=-1, keepdims=True) + EPS)
        out_ref[:, value] = (attended * scale * g_ref[:, value].astype(F32)).astype(BF16)


def gate_theirs(q, c, o, g):
    outs = [("vmem", g.shape, BF16)]
    return call(gated, outs, [IN_VMEM] * 4, (q, c, o, g), limit=8, flops=10**9)


def mine_body(
    q_ref, c_ref, o_ref, g_ref, wa_hbm, wb_hbm, out_ref, wb_ref, wa_ref, rows_buf, sems
):
    in_a = column_copies(wa_hbm, wa_ref, sems, 0)
    in_b = column_copies(wb_hbm, wb_ref, sems, len(in_a))
    for copy in in_a + in_b:
        copy.start()
    gated(q_ref, c_ref, o_ref, g_ref, rows_buf)
    for copy, cut in zip(in_a, blocks(wa_ref.shape[1])):
        copy.wait()
        out_ref[:, cut] = dot(rows_buf[...], wa_ref[:, cut])
    for copy in in_b:
        copy.wait()


def out_mine(q, c, o, g, wa, wb):
    rows = q.shape[0]
    depth, width = wa.shape
    return call(
        mine_body,
        [("vmem", (rows, width), F32), ("vmem", (depth, width // 2), BF16)],
        [IN_VMEM] * 4 + [IN_HBM] * 2,
        (q, c, o, g, wa, wb),
        scratch=[
            pltpu.VMEM((depth, width), BF16),
            pltpu.VMEM(g.shape, BF16),
            pltpu.SemaphoreType.DMA((2 * width // COLS,)),
        ],
        limit=32,
        flops=2 * rows * depth * width,
    )


def last_body(a_ref, w_ref, p_ref, wb_hbm, out_hbm, wb_ref, buf, in_sems, sems):
    width, here = buf.shape[1], w_ref.shape[1]
    more = []
    for i, c in enumerate(range(here, width, COLS)):
        copy = pltpu.make_async_copy(
            wb_hbm.at[:, pl.ds(c, COLS)], wb_ref.at[:, pl.ds(c - here, COLS)], in_sems.at[i]
        )
        copy.start()
        more.append(copy)
    copies = []
    for i, cut in enumerate(blocks(width)):
        if cut.start < here:
            w = w_ref[:, cut]
        else:
            more[i - here // COLS].wait()
            w = wb_ref[:, cut.start - here : cut.stop - here]
        buf[:, cut] = (p_ref[:, cut] + dot(a_ref[...], w)).astype(BF16)
        wide = pl.ds(i * COLS, COLS)
        copies.append(pltpu.make_async_copy(buf.at[:, wide], out_hbm.at[:, wide], sems.at[i]))
        copies[-1].start()
    for copy in copies:
        copy.wait()


def out_last(a, w, partial, wb):
    rows, width = partial.shape
    depth = w.shape[0]
    return call(
        last_body,
        [("hbm", (rows, width), BF16)],
        [IN_VMEM] * 3 + [IN_HBM],
        (a, w, partial, wb),
        scratch=[
            pltpu.VMEM((depth, width - w.shape[1]), BF16),
            pltpu.VMEM((rows, width), BF16),
            pltpu.SemaphoreType.DMA((width // COLS,)),
            pltpu.SemaphoreType.DMA((width // COLS,)),
        ],
        limit=20,
        flops=2 * rows * depth * width,
    )


def swap(x):
    return lax.ppermute(x, "tp", [(0, 1), (1, 0)])


def scalar(x):
    return x.astype(jnp.int32).reshape(1)


def mixer(tokens, norm_gain, wq, wk, wv, wg, decay_bias, head_gain, wo):
    rows = tokens.shape[0]
    kw = wk.shape[1]
    heads = kw // HEAD_K
    tp = lax.axis_index("tp").astype(jnp.int32)
    start = (lax.axis_index(SP) * (2 * rows)).astype(jnp.int32)
    at, bt = scalar(start + tp * rows), scalar(start + (1 - tp) * rows)
    sequence = lax.axis_size(SP) * 2 * rows
    bias = decay_bias.astype(F32).reshape(1, kw)
    gain = norm_gain.astype(F32).reshape(1, -1)
    out_gain = head_gain.astype(F32).reshape(1, -1)
    far = functools.partial(pltpu.with_memory_space_constraint, memory_space=pltpu.HBM)

    others = swap(tokens)
    xa, wk, wv, ka, va, sa = project_first(
        at, *map(far, (tokens, gain, bias, wk, wv)), sequence
    )
    xa, ka, va, xb, kb, vb, sb, state = project_second(
        bt, others, gain, bias, wk, wv, sa, xa, ka, va, sequence
    )
    other_wo = swap(wo)

    stretches = lax.axis_size(SP)
    pieces = state.reshape(stretches, heads * HEAD_K // stretches, HEAD_V)
    got = lax.all_to_all(pieces, SP, 0, 0, tiled=True)
    qa, qb, oa, ob = project_query(
        scalar(tp), at, bt, bias, sa, *map(far, (sb, ka, kb, va, vb, xa, xb, wq)), sequence
    )
    carried = lax.all_to_all(before_of(got), SP, 0, 0, tiled=True)
    ga, gb = project_gate(out_gain, far(xa), far(xb), far(wg))
    carried = carried.reshape(heads, HEAD_K, HEAD_V)

    theirs = gate_theirs(qb, carried, ob, gb)
    received = swap(theirs)
    partial, wb = out_mine(qa, carried, oa, ga, far(wo), far(other_wo))
    return out_last(received, wb, partial, far(other_wo))


def solution(mesh):
    z, y, x = 4, 4, 4
    finer = Mesh(mesh.devices.reshape(z, y, x, mesh.shape["tp"]), AXES)
    rows = P(AXES, None)
    cols = P(None, "tp")
    in_specs = (rows, P(), cols, cols, cols, cols, P("tp"), P("tp"), P("tp", None))
    return jax.shard_map(mixer, mesh=finer, in_specs=in_specs, out_specs=rows, check_vma=False)
```

```python
import functools
import math

import jax
import jax.numpy as jnp
from jax import lax
from jax.experimental import pallas as pl
from jax.experimental.pallas import tpu as pltpu
from jax.sharding import Mesh
from jax.sharding import PartitionSpec as P

HEAD_K = 128
HEAD_V = 256
AXES = ("z1", "z0", "y", "x", "tp")
SP = ("z1", "z0", "y", "x")
INNER = ("z0", "y", "x")
OUTER = "z1"
EPS = 1e-06
COLS = 512
STEP = 64
MIB = 1024 * 1024
F32 = jnp.float32
BF16 = jnp.bfloat16
IN_VMEM = pl.BlockSpec(memory_space=pltpu.VMEM)
IN_HBM = pl.BlockSpec(memory_space=pl.ANY)
IN_SMEM = pl.BlockSpec(memory_space=pltpu.SMEM)


def call(body, outs, in_specs, args, scratch=(), limit=16, flops=0):
    size = sum(a.size * a.dtype.itemsize for a in args)
    kinds = {"vmem": (pltpu.VMEM, IN_VMEM), "hbm": (pltpu.HBM, IN_HBM)}
    out_shape = tuple(kinds[k][0](dims, dtype) for k, dims, dtype in outs)
    run = pl.pallas_call(
        body,
        out_shape=out_shape,
        in_specs=in_specs,
        out_specs=tuple(kinds[k][1] for k, _, _ in outs),
        scratch_shapes=scratch,
        compiler_params=pltpu.CompilerParams(vmem_limit_bytes=limit * MIB),
        cost_estimate=pl.CostEstimate(flops=flops, bytes_accessed=size, transcendentals=0),
    )
    out = run(*args)
    return out if len(out) > 1 else out[0]


def dot(a, b):
    return jnp.dot(a, b, preferred_element_type=F32)


def blocks(width, size=COLS):
    return [slice(c, c + size) for c in range(0, width, size)]


def column_copies(src, dst, sems, first):
    return [
        pltpu.make_async_copy(
            src.at[:, pl.ds(c, COLS)], dst.at[:, pl.ds(c, COLS)], sems.at[first + i]
        )
        for i, c in enumerate(range(0, dst.shape[1], COLS))
    ]


def normalized(x, gain):
    x = x.astype(F32)
    scale = lax.rsqrt(jnp.mean(x * x, axis=-1, keepdims=True) + EPS)
    return (x * scale * gain).astype(BF16)


def log_decay(bias, sequence):
    logits = bias + math.log(sequence / 8.0)
    return -(jnp.maximum(-logits, 0.0) + jnp.log1p(jnp.exp(-jnp.abs(logits)))) / 16.0


def positions(start, rows):
    return (start + 1 + lax.broadcasted_iota(jnp.int32, (rows, COLS), 0)).astype(F32)


def put_keys(x, w, ld, position, k_ref, cut):
    k_ref[:, cut] = (dot(x, w) * jnp.exp(-ld[:, cut] * position)).astype(BF16)


def state_of(k_ref, v_ref, h):
    return lax.dot_general(
        k_ref[:, h * HEAD_K : (h + 1) * HEAD_K],
        v_ref[:, h * HEAD_V : (h + 1) * HEAD_V],
        (((0,), (0,)), ((), ())),
        preferred_element_type=F32,
    )


def first_body(
    start_ref, x_hbm, gain_hbm, bias_hbm, wk_hbm, wv_hbm, xn_ref, wk_ref, wv_ref, k_ref, v_ref,
    s_ref, buf, gain_ref, bias_ref, sems, *, sequence
):
    rows = buf.shape[0]
    small = [
        pltpu.make_async_copy(gain_hbm, gain_ref, sems.at[0]),
        pltpu.make_async_copy(bias_hbm, bias_ref, sems.at[1]),
    ]
    in_x = [
        pltpu.make_async_copy(
            x_hbm.at[pl.ds(r, STEP), :], buf.at[pl.ds(r, STEP), :], sems.at[2 + i]
        )
        for i, r in enumerate(range(0, rows, STEP))
    ]
    in_k = column_copies(wk_hbm, wk_ref, sems, 2 + len(in_x))
    in_v = column_copies(wv_hbm, wv_ref, sems, 2 + len(in_x) + len(in_k))
    for copy in small + in_x + in_k + in_v:
        copy.start()
    for copy in small:
        copy.wait()
    ld = log_decay(bias_ref[...], sequence)
    for i, copy in enumerate(in_x):
        copy.wait()
        cut = slice(i * STEP, (i + 1) * STEP)
        xn_ref[cut, :] = normalized(buf[cut, :], gain_ref[...])
    position = positions(start_ref[0], rows)
    for copy, cut in zip(in_k, blocks(wk_ref.shape[1])):
        copy.wait()
        put_keys(xn_ref[...], wk_ref[:, cut], ld, position, k_ref, cut)
    for copy, cut in zip(in_v, blocks(wv_ref.shape[1])):
        copy.wait()
        v_ref[:, cut] = dot(xn_ref[...], wv_ref[:, cut]).astype(BF16)
    for h in range(s_ref.shape[0]):
        s_ref[h] = state_of(k_ref, v_ref, h)


def project_first(start, x, gain, bias, wk, wv, sequence):
    rows, depth = x.shape
    kw, vw = wk.shape[1], wv.shape[1]
    heads = kw // HEAD_K
    return call(
        functools.partial(first_body, sequence=sequence),
        [
            ("vmem", (rows, depth), BF16),
            ("vmem", (depth, kw), BF16),
            ("vmem", (depth, vw), BF16),
            ("vmem", (rows, kw), BF16),
            ("vmem", (rows, vw), BF16),
            ("vmem", (heads, HEAD_K, HEAD_V), F32),
        ],
        [IN_SMEM] + [IN_HBM] * 5,
        (start, x, gain, bias, wk, wv),
        scratch=[
            pltpu.VMEM((rows, depth), BF16),
            pltpu.VMEM(gain.shape, F32),
            pltpu.VMEM(bias.shape, F32),
            pltpu.SemaphoreType.DMA((2 + rows // STEP + (kw + vw) // COLS,)),
        ],
        limit=24,
        flops=2 * rows * depth * (kw + vw),
    )


def second_body(
    start_ref, late_ref, x_ref, gain_ref, bias_ref, wk_ref, wv_ref, prev_ref, xa_ref, ka_ref, va_ref,
    xa_hbm, ka_hbm, va_hbm, xn_hbm, k_hbm, v_hbm, s_hbm, sum_hbm, xn_ref, k_ref, v_ref, s_ref,
    sum_buf, sems, *, sequence
):
    rows = x_ref.shape[0]
    heads = s_ref.shape[0]
    out = []

    def send(src, dst):
        out.append(pltpu.make_async_copy(src, dst, sems.at[len(out)]))
        out[-1].start()

    send(ka_ref, ka_hbm)
    send(va_ref, va_hbm)
    send(xa_ref, xa_hbm)
    ld = log_decay(bias_ref[...], sequence)
    for cut in blocks(rows, STEP):
        xn_ref[cut, :] = normalized(x_ref[cut, :], gain_ref[...])
    send(xn_ref, xn_hbm)
    position = positions(start_ref[0], rows)
    for cut in blocks(wk_ref.shape[1]):
        put_keys(xn_ref[...], wk_ref[:, cut], ld, position, k_ref, cut)
    for cut in blocks(wv_ref.shape[1]):
        v_ref[:, cut] = dot(xn_ref[...], wv_ref[:, cut]).astype(BF16)
    for h in range(heads):
        state = state_of(k_ref, v_ref, h)
        s_ref[h] = state.astype(BF16)
        sum_buf[h] = (state + prev_ref[h]).astype(BF16)
        send(sum_buf.at[h], sum_hbm.at[(h + late_ref[0] * (heads // 2)) % heads])
    send(s_ref, s_hbm)
    send(k_ref, k_hbm)
    send(v_ref, v_hbm)
    for copy in out:
        copy.wait()


def project_second(start, late, x, gain, bias, wk, wv, before, xa, ka, va, sequence):
    rows, depth = x.shape
    kw, vw = wk.shape[1], wv.shape[1]
    heads = kw // HEAD_K
    half = [("hbm", (rows, depth), BF16), ("hbm", (rows, kw), BF16), ("hbm", (rows, vw), BF16)]
    return call(
        functools.partial(second_body, sequence=sequence),
        half
        + half
        + [("hbm", (heads, HEAD_K, HEAD_V), BF16)] * 2,
        [IN_SMEM] * 2 + [IN_VMEM] * 9,
        (start, late, x, gain, bias, wk, wv, before, xa, ka, va),
        scratch=[
            pltpu.VMEM((rows, depth), BF16),
            pltpu.VMEM((rows, kw), BF16),
            pltpu.VMEM((rows, vw), BF16),
            pltpu.VMEM((heads, HEAD_K, HEAD_V), BF16),
            pltpu.VMEM((heads, HEAD_K, HEAD_V), BF16),
            pltpu.SemaphoreType.DMA((7 + heads,)),
        ],
        limit=28,
        flops=2 * rows * depth * (kw + vw),
    )


def query_body(
    tp_ref, at_ref, bt_ref, bias_ref, sa_ref, sb_hbm, ka_hbm, kb_hbm, va_hbm, vb_hbm, xa_hbm,
    xb_hbm, w_hbm, qa_ref, qb_ref, oa_ref, ob_ref, xa_ref, xb_ref, w_ref, ka_ref, kb_ref, va_ref,
    vb_ref, sb_ref, sems, *, sequence
):
    copies = [
        pltpu.make_async_copy(src, dst, sems.at[i])
        for i, (src, dst) in enumerate(
            (
                (xa_hbm, xa_ref),
                (w_hbm, w_ref),
                (ka_hbm, ka_ref),
                (va_hbm, va_ref),
                (sb_hbm, sb_ref),
                (xb_hbm, xb_ref),
                (kb_hbm, kb_ref),
                (vb_hbm, vb_ref),
            )
        )
    ]
    for copy in copies:
        copy.start()
    upper = tp_ref[0].astype(F32)
    halves = (
        (at_ref, xa_ref, ka_ref, va_ref, qa_ref, oa_ref, sb_ref, upper, copies[:5]),
        (bt_ref, xb_ref, kb_ref, vb_ref, qb_ref, ob_ref, sa_ref, 1.0 - upper, copies[5:]),
    )
    rows = xa_ref.shape[0]
    ld = log_decay(bias_ref[...], sequence)
    keep = lax.broadcasted_iota(jnp.int32, (rows, rows), 0) >= lax.broadcasted_iota(
        jnp.int32, (rows, rows), 1
    )
    for start, x_ref, k_ref, v_ref, q_ref, o_ref, s_ref, later, needs in halves:
        for copy in needs:
            copy.wait()
        for cut in blocks(w_ref.shape[1]):
            decay = jnp.exp(ld[:, cut] * positions(start[0], rows)) * HEAD_K ** (-0.5)
            q_ref[:, cut] = (dot(x_ref[...], w_ref[:, cut]) * decay).astype(BF16)
        for h in range(w_ref.shape[1] // HEAD_K):
            key = slice(h * HEAD_K, (h + 1) * HEAD_K)
            value = slice(h * HEAD_V, (h + 1) * HEAD_V)
            scores = lax.dot_general(
                q_ref[:, key], k_ref[:, key], (((1,), (1,)), ((), ())), preferred_element_type=F32
            )
            scores = jnp.where(keep, scores, 0.0).astype(BF16)
            earlier = (s_ref[h].astype(F32) * later).astype(BF16)
            local = dot(scores, v_ref[:, value]) + dot(q_ref[:, key], earlier)
            o_ref[:, value] = local.astype(BF16)


def project_query(tp, at, bt, bias, sa, sb, ka, kb, va, vb, xa, xb, w, sequence):
    rows, depth = xa.shape
    kw, vw = w.shape[1], va.shape[1]
    return call(
        functools.partial(query_body, sequence=sequence),
        [
            ("vmem", (rows, kw), BF16),
            ("vmem", (rows, kw), BF16),
            ("vmem", (rows, vw), BF16),
            ("vmem", (rows, vw), BF16),
        ],
        [IN_SMEM] * 3 + [IN_VMEM] * 2 + [IN_HBM] * 8,
        (tp, at, bt, bias, sa, sb, ka, kb, va, vb, xa, xb, w),
        scratch=[
            pltpu.VMEM((rows, depth), BF16),
            pltpu.VMEM((rows, depth), BF16),
            pltpu.VMEM((depth, kw), BF16),
            pltpu.VMEM((rows, kw), BF16),
            pltpu.VMEM((rows, kw), BF16),
            pltpu.VMEM((rows, vw), BF16),
            pltpu.VMEM((rows, vw), BF16),
            pltpu.VMEM(sb.shape, BF16),
            pltpu.SemaphoreType.DMA((8,)),
        ],
        limit=32,
        flops=5 * rows * depth * kw,
    )


def gate_body(gain_ref, xa_hbm, xb_hbm, w_hbm, ga_ref, gb_ref, xa_ref, xb_ref, w_ref, sems):
    in_a = pltpu.make_async_copy(xa_hbm, xa_ref, sems.at[0])
    in_b = pltpu.make_async_copy(xb_hbm, xb_ref, sems.at[1])
    in_w = column_copies(w_hbm, w_ref, sems, 2)
    for copy in [in_a, in_w[0], in_b] + in_w[1:]:
        copy.start()
    in_a.wait()
    for i, (copy, cut) in enumerate(zip(in_w, blocks(w_ref.shape[1]))):
        copy.wait()
        for x_ref, g_ref in ((xa_ref, ga_ref), (xb_ref, gb_ref)):
            if i == 0 and x_ref is xb_ref:
                in_b.wait()
            acc = dot(x_ref[...], w_ref[:, cut])
            g_ref[:, cut] = (acc * gain_ref[:, cut] / (1.0 + jnp.exp(-acc))).astype(BF16)


def project_gate(gain, xa, xb, w):
    rows, depth = xa.shape
    width = w.shape[1]
    return call(
        gate_body,
        [("vmem", (rows, width), BF16), ("vmem", (rows, width), BF16)],
        [IN_VMEM] + [IN_HBM] * 3,
        (gain, xa, xb, w),
        scratch=[
            pltpu.VMEM((rows, depth), BF16),
            pltpu.VMEM((rows, depth), BF16),
            pltpu.VMEM((depth, width), BF16),
            pltpu.SemaphoreType.DMA((2 + width // COLS,)),
        ],
        limit=32,
        flops=4 * rows * depth * width,
    )


def total_body(got_ref, out_ref):
    total = got_ref[0].astype(F32)
    for j in range(1, got_ref.shape[0]):
        total = total + got_ref[j].astype(F32)
    out_ref[...] = total.astype(BF16)


def total_of(got):
    return call(total_body, [("vmem", got.shape[1:], BF16)], [IN_VMEM], (got,), limit=4)


def before_body(late_ref, tp_ref, got_ref, far_ref, out_hbm, out_ref, sems):
    count = got_ref.shape[0]
    run = far_ref[...].astype(F32) * late_ref[0].astype(F32)
    for j in range(count):
        slot = j + tp_ref[0] * (count - 1 - 2 * j)
        out_ref[slot] = run.astype(BF16)
        run = run + got_ref[slot].astype(F32)
    copy = pltpu.make_async_copy(out_ref, out_hbm, sems.at[0])
    copy.start()
    copy.wait()


def before_of(late, tp, got, far):
    return call(
        before_body,
        [("hbm", got.shape, BF16)],
        [IN_SMEM, IN_SMEM, IN_VMEM, IN_VMEM],
        (late, tp, got, far),
        scratch=[pltpu.VMEM(got.shape, BF16), pltpu.SemaphoreType.DMA((1,))],
        limit=4,
    )


def gated(late_ref, q_ref, c_ref, o_ref, g_ref, out_ref):
    heads = c_ref.shape[0]
    for h in range(heads):
        carried = c_ref[(h + late_ref[0] * (heads // 2)) % heads]
        key = slice(h * HEAD_K, (h + 1) * HEAD_K)
        value = slice(h * HEAD_V, (h + 1) * HEAD_V)
        attended = o_ref[:, value].astype(F32) + dot(q_ref[:, key], carried)
        scale = lax.rsqrt(jnp.mean(attended * attended, axis=-1, keepdims=True) + EPS)
        out_ref[:, value] = (attended * scale * g_ref[:, value].astype(F32)).astype(BF16)


def gate_theirs(late, q, c, o, g):
    outs = [("vmem", g.shape, BF16)]
    specs = [IN_SMEM] + [IN_VMEM] * 4
    return call(gated, outs, specs, (late, q, c, o, g), limit=8, flops=10**9)


def mine_body(
    late_ref, q_ref, c_ref, o_ref, g_ref, wa_hbm, wb_hbm, out_ref, wb_ref, wa_ref, rows_buf, sems
):
    in_a = column_copies(wa_hbm, wa_ref, sems, 0)
    in_b = column_copies(wb_hbm, wb_ref, sems, len(in_a))
    for copy in in_a + in_b:
        copy.start()
    gated(late_ref, q_ref, c_ref, o_ref, g_ref, rows_buf)
    for copy, cut in zip(in_a, blocks(wa_ref.shape[1])):
        copy.wait()
        out_ref[:, cut] = dot(rows_buf[...], wa_ref[:, cut])
    for copy in in_b:
        copy.wait()


def out_mine(late, q, c, o, g, wa, wb):
    rows = q.shape[0]
    depth, width = wa.shape
    return call(
        mine_body,
        [("vmem", (rows, width), F32), ("vmem", (depth, width // 2), BF16)],
        [IN_SMEM] + [IN_VMEM] * 4 + [IN_HBM] * 2,
        (late, q, c, o, g, wa, wb),
        scratch=[
            pltpu.VMEM((depth, width), BF16),
            pltpu.VMEM(g.shape, BF16),
            pltpu.SemaphoreType.DMA((2 * width // COLS,)),
        ],
        limit=32,
        flops=2 * rows * depth * width,
    )


def last_body(a_ref, w_ref, p_ref, wb_hbm, out_hbm, wb_ref, buf, in_sems, sems):
    width, here = buf.shape[1], w_ref.shape[1]
    more = []
    for i, c in enumerate(range(here, width, COLS)):
        copy = pltpu.make_async_copy(
            wb_hbm.at[:, pl.ds(c, COLS)], wb_ref.at[:, pl.ds(c - here, COLS)], in_sems.at[i]
        )
        copy.start()
        more.append(copy)
    copies = []
    for i, cut in enumerate(blocks(width)):
        if cut.start < here:
            w = w_ref[:, cut]
        else:
            more[i - here // COLS].wait()
            w = wb_ref[:, cut.start - here : cut.stop - here]
        buf[:, cut] = (p_ref[:, cut] + dot(a_ref[...], w)).astype(BF16)
        wide = pl.ds(i * COLS, COLS)
        copies.append(pltpu.make_async_copy(buf.at[:, wide], out_hbm.at[:, wide], sems.at[i]))
        copies[-1].start()
    for copy in copies:
        copy.wait()


def out_last(a, w, partial, wb):
    rows, width = partial.shape
    depth = w.shape[0]
    return call(
        last_body,
        [("hbm", (rows, width), BF16)],
        [IN_VMEM] * 3 + [IN_HBM],
        (a, w, partial, wb),
        scratch=[
            pltpu.VMEM((depth, width - w.shape[1]), BF16),
            pltpu.VMEM((rows, width), BF16),
            pltpu.SemaphoreType.DMA((width // COLS,)),
            pltpu.SemaphoreType.DMA((width // COLS,)),
        ],
        limit=20,
        flops=2 * rows * depth * width,
    )


def swap(x):
    return lax.ppermute(x, "tp", [(0, 1), (1, 0)])


def exchange(pieces):
    halves, members, cores = lax.axis_size(OUTER), lax.axis_size(INNER), lax.axis_size("tp")
    groups = []
    for half in range(halves):
        for core in range(cores):
            group = [(half * members + j) * cores + core for j in range(members)]
            groups.append(group[::-1] if core else group)
    return lax.all_to_all(pieces, AXES, 0, 0, axis_index_groups=groups, tiled=True)


def scalar(x):
    return x.astype(jnp.int32).reshape(1)


def mixer(tokens, norm_gain, wq, wk, wv, wg, decay_bias, head_gain, wo):
    rows = tokens.shape[0]
    kw = wk.shape[1]
    heads = kw // HEAD_K
    tp = lax.axis_index("tp").astype(jnp.int32)
    start = (lax.axis_index(SP) * (2 * rows)).astype(jnp.int32)
    at, bt = scalar(start + tp * rows), scalar(start + (1 - tp) * rows)
    sequence = lax.axis_size(SP) * 2 * rows
    bias = decay_bias.astype(F32).reshape(1, kw)
    gain = norm_gain.astype(F32).reshape(1, -1)
    out_gain = head_gain.astype(F32).reshape(1, -1)
    far = functools.partial(pltpu.with_memory_space_constraint, memory_space=pltpu.HBM)

    late = scalar(lax.axis_index(OUTER))
    others = swap(tokens)
    xa, wk, wv, ka, va, sa = project_first(
        at, *map(far, (tokens, gain, bias, wk, wv)), sequence
    )
    xa, ka, va, xb, kb, vb, sb, state = project_second(
        bt, late, others, gain, bias, wk, wv, sa, xa, ka, va, sequence
    )
    other_wo = swap(wo)

    stretches = lax.axis_size(INNER)
    pieces = state.reshape(stretches, heads * HEAD_K // stretches, HEAD_V)
    got = exchange(pieces)
    qa, qb, oa, ob = project_query(
        scalar(tp), at, bt, bias, sa, *map(far, (sb, ka, kb, va, vb, xa, xb, wq)), sequence
    )
    planes = lax.axis_size(("z1", "z0"))
    mirror = [(i, planes - 1 - i) for i in range(planes)]
    other_total = lax.ppermute(total_of(got), ("z1", "z0"), mirror)
    before = before_of(late, scalar(tp), got, other_total)
    carried = exchange(before)
    ga, gb = project_gate(out_gain, far(xa), far(xb), far(wg))
    carried = carried.reshape(heads, HEAD_K, HEAD_V)

    theirs = gate_theirs(late, qb, carried, ob, gb)
    received = swap(theirs)
    partial, wb = out_mine(late, qa, carried, oa, ga, far(wo), far(other_wo))
    return out_last(received, wb, partial, far(other_wo))


def solution(mesh):
    finer = Mesh(mesh.devices.reshape(2, 2, 4, 4, mesh.shape["tp"]), AXES)
    rows = P(AXES, None)
    cols = P(None, "tp")
    in_specs = (rows, P(), cols, cols, cols, cols, P("tp"), P("tp"), P("tp", None))
    return jax.shard_map(mixer, mesh=finer, in_specs=in_specs, out_specs=rows, check_vma=False)
```

```python
import functools
import math

import jax
import jax.numpy as jnp
from jax import lax
from jax.experimental import pallas as pl
from jax.experimental.pallas import tpu as pltpu
from jax.sharding import Mesh
from jax.sharding import PartitionSpec as P

HEAD_K = 128
HEAD_V = 256
AXES = ("z1", "z0", "y", "x", "tp")
SP = ("z1", "z0", "y", "x")
INNER = ("z0", "y", "x")
OUTER = "z1"
EPS = 1e-06
COLS = 512
STEP = 64
MIB = 1024 * 1024
F32 = jnp.float32
BF16 = jnp.bfloat16
IN_VMEM = pl.BlockSpec(memory_space=pltpu.VMEM)
IN_HBM = pl.BlockSpec(memory_space=pl.ANY)
IN_SMEM = pl.BlockSpec(memory_space=pltpu.SMEM)


def call(body, outs, in_specs, args, scratch=(), limit=16, flops=0):
    size = sum(a.size * a.dtype.itemsize for a in args)
    kinds = {"vmem": (pltpu.VMEM, IN_VMEM), "hbm": (pltpu.HBM, IN_HBM)}
    out_shape = tuple(kinds[k][0](dims, dtype) for k, dims, dtype in outs)
    run = pl.pallas_call(
        body,
        out_shape=out_shape,
        in_specs=in_specs,
        out_specs=tuple(kinds[k][1] for k, _, _ in outs),
        scratch_shapes=scratch,
        compiler_params=pltpu.CompilerParams(vmem_limit_bytes=limit * MIB),
        cost_estimate=pl.CostEstimate(flops=flops, bytes_accessed=size, transcendentals=0),
    )
    out = run(*args)
    return out if len(out) > 1 else out[0]


def dot(a, b):
    return jnp.dot(a, b, preferred_element_type=F32)


def blocks(width, size=COLS):
    return [slice(c, c + size) for c in range(0, width, size)]


def column_copies(src, dst, sems, first):
    return [
        pltpu.make_async_copy(
            src.at[:, pl.ds(c, COLS)], dst.at[:, pl.ds(c, COLS)], sems.at[first + i]
        )
        for i, c in enumerate(range(0, dst.shape[1], COLS))
    ]


def normalized(x, gain):
    x = x.astype(F32)
    scale = lax.rsqrt(jnp.mean(x * x, axis=-1, keepdims=True) + EPS)
    return (x * scale * gain).astype(BF16)


def log_decay(bias, sequence):
    logits = bias + math.log(sequence / 8.0)
    return -(jnp.maximum(-logits, 0.0) + jnp.log1p(jnp.exp(-jnp.abs(logits)))) / 16.0


def positions(start, rows):
    return (start + 1 + lax.broadcasted_iota(jnp.int32, (rows, COLS), 0)).astype(F32)


def put_keys(x, w, ld, position, k_ref, cut):
    k_ref[:, cut] = (dot(x, w) * jnp.exp(-ld[:, cut] * position)).astype(BF16)


def state_of(k_ref, v_ref, h):
    return lax.dot_general(
        k_ref[:, h * HEAD_K : (h + 1) * HEAD_K],
        v_ref[:, h * HEAD_V : (h + 1) * HEAD_V],
        (((0,), (0,)), ((), ())),
        preferred_element_type=F32,
    )


def first_body(
    start_ref, x_hbm, gain_hbm, bias_hbm, wk_hbm, wv_hbm, xn_ref, wk_ref, wv_ref, k_ref, v_ref,
    s_ref, buf, gain_ref, bias_ref, sems, *, sequence
):
    rows = buf.shape[0]
    small = [
        pltpu.make_async_copy(gain_hbm, gain_ref, sems.at[0]),
        pltpu.make_async_copy(bias_hbm, bias_ref, sems.at[1]),
    ]
    in_x = [
        pltpu.make_async_copy(
            x_hbm.at[pl.ds(r, STEP), :], buf.at[pl.ds(r, STEP), :], sems.at[2 + i]
        )
        for i, r in enumerate(range(0, rows, STEP))
    ]
    in_k = column_copies(wk_hbm, wk_ref, sems, 2 + len(in_x))
    in_v = column_copies(wv_hbm, wv_ref, sems, 2 + len(in_x) + len(in_k))
    for copy in small + in_x + in_k + in_v:
        copy.start()
    for copy in small:
        copy.wait()
    ld = log_decay(bias_ref[...], sequence)
    for i, copy in enumerate(in_x):
        copy.wait()
        cut = slice(i * STEP, (i + 1) * STEP)
        xn_ref[cut, :] = normalized(buf[cut, :], gain_ref[...])
    position = positions(start_ref[0], rows)
    for copy, cut in zip(in_k, blocks(wk_ref.shape[1])):
        copy.wait()
        put_keys(xn_ref[...], wk_ref[:, cut], ld, position, k_ref, cut)
    for copy, cut in zip(in_v, blocks(wv_ref.shape[1])):
        copy.wait()
        v_ref[:, cut] = dot(xn_ref[...], wv_ref[:, cut]).astype(BF16)
    for h in range(s_ref.shape[0]):
        s_ref[h] = state_of(k_ref, v_ref, h)


def project_first(start, x, gain, bias, wk, wv, sequence):
    rows, depth = x.shape
    kw, vw = wk.shape[1], wv.shape[1]
    heads = kw // HEAD_K
    return call(
        functools.partial(first_body, sequence=sequence),
        [
            ("vmem", (rows, depth), BF16),
            ("vmem", (depth, kw), BF16),
            ("vmem", (depth, vw), BF16),
            ("vmem", (rows, kw), BF16),
            ("vmem", (rows, vw), BF16),
            ("vmem", (heads, HEAD_K, HEAD_V), F32),
        ],
        [IN_SMEM] + [IN_HBM] * 5,
        (start, x, gain, bias, wk, wv),
        scratch=[
            pltpu.VMEM((rows, depth), BF16),
            pltpu.VMEM(gain.shape, F32),
            pltpu.VMEM(bias.shape, F32),
            pltpu.SemaphoreType.DMA((2 + rows // STEP + (kw + vw) // COLS,)),
        ],
        limit=24,
        flops=2 * rows * depth * (kw + vw),
    )


def second_body(
    start_ref, late_ref, x_ref, gain_ref, bias_ref, wk_ref, wv_ref, prev_ref, xa_ref, ka_ref, va_ref,
    xa_hbm, ka_hbm, va_hbm, xn_hbm, k_hbm, v_hbm, s_hbm, sum_hbm, xn_ref, k_ref, v_ref, s_ref,
    sum_buf, sems, *, sequence
):
    rows = x_ref.shape[0]
    heads = s_ref.shape[0]
    out = []

    def send(src, dst):
        out.append(pltpu.make_async_copy(src, dst, sems.at[len(out)]))
        out[-1].start()

    send(ka_ref, ka_hbm)
    send(va_ref, va_hbm)
    send(xa_ref, xa_hbm)
    ld = log_decay(bias_ref[...], sequence)
    for cut in blocks(rows, STEP):
        xn_ref[cut, :] = normalized(x_ref[cut, :], gain_ref[...])
    send(xn_ref, xn_hbm)
    position = positions(start_ref[0], rows)
    for cut in blocks(wk_ref.shape[1]):
        put_keys(xn_ref[...], wk_ref[:, cut], ld, position, k_ref, cut)
    send(k_ref, k_hbm)
    for cut in blocks(wv_ref.shape[1]):
        v_ref[:, cut] = dot(xn_ref[...], wv_ref[:, cut]).astype(BF16)
    for h in range(heads):
        state = state_of(k_ref, v_ref, h)
        s_ref[h] = state.astype(BF16)
        sum_buf[h] = (state + prev_ref[h]).astype(BF16)
        send(sum_buf.at[h], sum_hbm.at[(h + late_ref[0] * (heads // 2)) % heads])
    send(s_ref, s_hbm)
    send(v_ref, v_hbm)
    for copy in out:
        copy.wait()


def project_second(start, late, x, gain, bias, wk, wv, before, xa, ka, va, sequence):
    rows, depth = x.shape
    kw, vw = wk.shape[1], wv.shape[1]
    heads = kw // HEAD_K
    half = [("hbm", (rows, depth), BF16), ("hbm", (rows, kw), BF16), ("hbm", (rows, vw), BF16)]
    return call(
        functools.partial(second_body, sequence=sequence),
        half
        + half
        + [("hbm", (heads, HEAD_K, HEAD_V), BF16)] * 2,
        [IN_SMEM] * 2 + [IN_VMEM] * 9,
        (start, late, x, gain, bias, wk, wv, before, xa, ka, va),
        scratch=[
            pltpu.VMEM((rows, depth), BF16),
            pltpu.VMEM((rows, kw), BF16),
            pltpu.VMEM((rows, vw), BF16),
            pltpu.VMEM((heads, HEAD_K, HEAD_V), BF16),
            pltpu.VMEM((heads, HEAD_K, HEAD_V), BF16),
            pltpu.SemaphoreType.DMA((7 + heads,)),
        ],
        limit=28,
        flops=2 * rows * depth * (kw + vw),
    )


def query_body(
    tp_ref, at_ref, bt_ref, bias_ref, sa_ref, sb_hbm, ka_hbm, kb_hbm, va_hbm, vb_hbm, xa_hbm,
    xb_hbm, w_hbm, qa_ref, qb_ref, oa_ref, ob_ref, xa_ref, xb_ref, w_ref, ka_ref, kb_ref, va_ref,
    vb_ref, sb_ref, sems, *, sequence
):
    copies = [
        pltpu.make_async_copy(src, dst, sems.at[i])
        for i, (src, dst) in enumerate(
            (
                (xa_hbm, xa_ref),
                (w_hbm, w_ref),
                (ka_hbm, ka_ref),
                (va_hbm, va_ref),
                (sb_hbm, sb_ref),
                (xb_hbm, xb_ref),
                (kb_hbm, kb_ref),
                (vb_hbm, vb_ref),
            )
        )
    ]
    for copy in copies:
        copy.start()
    upper = tp_ref[0].astype(F32)
    halves = (
        (at_ref, xa_ref, ka_ref, va_ref, qa_ref, oa_ref, sb_ref, upper, copies[:5]),
        (bt_ref, xb_ref, kb_ref, vb_ref, qb_ref, ob_ref, sa_ref, 1.0 - upper, copies[5:]),
    )
    rows = xa_ref.shape[0]
    ld = log_decay(bias_ref[...], sequence)
    keep = lax.broadcasted_iota(jnp.int32, (rows, rows), 0) >= lax.broadcasted_iota(
        jnp.int32, (rows, rows), 1
    )
    for start, x_ref, k_ref, v_ref, q_ref, o_ref, s_ref, later, needs in halves:
        for copy in needs:
            copy.wait()
        for cut in blocks(w_ref.shape[1]):
            decay = jnp.exp(ld[:, cut] * positions(start[0], rows)) * HEAD_K ** (-0.5)
            q_ref[:, cut] = (dot(x_ref[...], w_ref[:, cut]) * decay).astype(BF16)
        for h in range(w_ref.shape[1] // HEAD_K):
            key = slice(h * HEAD_K, (h + 1) * HEAD_K)
            value = slice(h * HEAD_V, (h + 1) * HEAD_V)
            scores = lax.dot_general(
                q_ref[:, key], k_ref[:, key], (((1,), (1,)), ((), ())), preferred_element_type=F32
            )
            scores = jnp.where(keep, scores, 0.0).astype(BF16)
            earlier = (s_ref[h].astype(F32) * later).astype(BF16)
            local = dot(scores, v_ref[:, value]) + dot(q_ref[:, key], earlier)
            o_ref[:, value] = local.astype(BF16)


def project_query(tp, at, bt, bias, sa, sb, ka, kb, va, vb, xa, xb, w, sequence):
    rows, depth = xa.shape
    kw, vw = w.shape[1], va.shape[1]
    return call(
        functools.partial(query_body, sequence=sequence),
        [
            ("vmem", (rows, kw), BF16),
            ("vmem", (rows, kw), BF16),
            ("vmem", (rows, vw), BF16),
            ("vmem", (rows, vw), BF16),
        ],
        [IN_SMEM] * 3 + [IN_VMEM] * 2 + [IN_HBM] * 8,
        (tp, at, bt, bias, sa, sb, ka, kb, va, vb, xa, xb, w),
        scratch=[
            pltpu.VMEM((rows, depth), BF16),
            pltpu.VMEM((rows, depth), BF16),
            pltpu.VMEM((depth, kw), BF16),
            pltpu.VMEM((rows, kw), BF16),
            pltpu.VMEM((rows, kw), BF16),
            pltpu.VMEM((rows, vw), BF16),
            pltpu.VMEM((rows, vw), BF16),
            pltpu.VMEM(sb.shape, BF16),
            pltpu.SemaphoreType.DMA((8,)),
        ],
        limit=32,
        flops=5 * rows * depth * kw,
    )


def gate_body(gain_ref, xa_hbm, xb_hbm, w_hbm, ga_ref, gb_ref, xa_ref, xb_ref, w_ref, sems):
    in_a = pltpu.make_async_copy(xa_hbm, xa_ref, sems.at[0])
    in_b = pltpu.make_async_copy(xb_hbm, xb_ref, sems.at[1])
    in_w = column_copies(w_hbm, w_ref, sems, 2)
    for copy in [in_a, in_w[0], in_b] + in_w[1:]:
        copy.start()
    in_a.wait()
    for i, (copy, cut) in enumerate(zip(in_w, blocks(w_ref.shape[1]))):
        copy.wait()
        for x_ref, g_ref in ((xa_ref, ga_ref), (xb_ref, gb_ref)):
            if i == 0 and x_ref is xb_ref:
                in_b.wait()
            acc = dot(x_ref[...], w_ref[:, cut])
            g_ref[:, cut] = (acc * gain_ref[:, cut] / (1.0 + jnp.exp(-acc))).astype(BF16)


def project_gate(gain, xa, xb, w):
    rows, depth = xa.shape
    width = w.shape[1]
    return call(
        gate_body,
        [("vmem", (rows, width), BF16), ("vmem", (rows, width), BF16)],
        [IN_VMEM] + [IN_HBM] * 3,
        (gain, xa, xb, w),
        scratch=[
            pltpu.VMEM((rows, depth), BF16),
            pltpu.VMEM((rows, depth), BF16),
            pltpu.VMEM((depth, width), BF16),
            pltpu.SemaphoreType.DMA((2 + width // COLS,)),
        ],
        limit=32,
        flops=4 * rows * depth * width,
    )


def total_body(got_ref, out_ref):
    total = got_ref[0].astype(F32)
    for j in range(1, got_ref.shape[0]):
        total = total + got_ref[j].astype(F32)
    out_ref[...] = total.astype(BF16)


def total_of(got):
    return call(total_body, [("vmem", got.shape[1:], BF16)], [IN_VMEM], (got,), limit=4)


def before_body(late_ref, got_ref, far_ref, out_hbm, out_ref, sems):
    parts = sems.shape[0]
    count = got_ref.shape[0] // parts
    run = far_ref[...].astype(F32) * late_ref[0].astype(F32)
    copies = []
    for i in range(parts):
        for j in range(i * count, (i + 1) * count):
            out_ref[j] = run.astype(BF16)
            run = run + got_ref[j].astype(F32)
        part = pl.ds(i * count, count)
        copies.append(pltpu.make_async_copy(out_ref.at[part], out_hbm.at[part], sems.at[i]))
        copies[-1].start()
    for copy in copies:
        copy.wait()


def before_of(late, got, far):
    return call(
        before_body,
        [("hbm", got.shape, BF16)],
        [IN_SMEM, IN_VMEM, IN_VMEM],
        (late, got, far),
        scratch=[pltpu.VMEM(got.shape, BF16), pltpu.SemaphoreType.DMA((4,))],
        limit=4,
    )


def gated(late_ref, q_ref, c_ref, o_ref, g_ref, out_ref):
    heads = c_ref.shape[0]
    for h in range(heads):
        carried = c_ref[(h + late_ref[0] * (heads // 2)) % heads]
        key = slice(h * HEAD_K, (h + 1) * HEAD_K)
        value = slice(h * HEAD_V, (h + 1) * HEAD_V)
        attended = o_ref[:, value].astype(F32) + dot(q_ref[:, key], carried)
        scale = lax.rsqrt(jnp.mean(attended * attended, axis=-1, keepdims=True) + EPS)
        out_ref[:, value] = (attended * scale * g_ref[:, value].astype(F32)).astype(BF16)


def gate_theirs(late, q, c, o, g):
    outs = [("vmem", g.shape, BF16)]
    specs = [IN_SMEM] + [IN_VMEM] * 4
    return call(gated, outs, specs, (late, q, c, o, g), limit=8, flops=10**9)


def mine_body(
    late_ref, q_ref, c_ref, o_ref, g_ref, wa_hbm, wb_hbm, out_ref, wb_ref, wa_ref, rows_buf, sems
):
    in_a = column_copies(wa_hbm, wa_ref, sems, 0)
    in_b = column_copies(wb_hbm, wb_ref, sems, len(in_a))
    for copy in in_a + in_b:
        copy.start()
    gated(late_ref, q_ref, c_ref, o_ref, g_ref, rows_buf)
    for copy, cut in zip(in_a, blocks(wa_ref.shape[1])):
        copy.wait()
        out_ref[:, cut] = dot(rows_buf[...], wa_ref[:, cut])
    for copy in in_b:
        copy.wait()


def out_mine(late, q, c, o, g, wa, wb):
    rows = q.shape[0]
    depth, width = wa.shape
    return call(
        mine_body,
        [("vmem", (rows, width), F32), ("vmem", (depth, width // 2), BF16)],
        [IN_SMEM] + [IN_VMEM] * 4 + [IN_HBM] * 2,
        (late, q, c, o, g, wa, wb),
        scratch=[
            pltpu.VMEM((depth, width), BF16),
            pltpu.VMEM(g.shape, BF16),
            pltpu.SemaphoreType.DMA((2 * width // COLS,)),
        ],
        limit=32,
        flops=2 * rows * depth * width,
    )


def last_body(a_ref, w_ref, p_ref, wb_hbm, out_hbm, wb_ref, buf, in_sems, sems):
    width, here = buf.shape[1], w_ref.shape[1]
    more = []
    for i, c in enumerate(range(here, width, COLS)):
        copy = pltpu.make_async_copy(
            wb_hbm.at[:, pl.ds(c, COLS)], wb_ref.at[:, pl.ds(c - here, COLS)], in_sems.at[i]
        )
        copy.start()
        more.append(copy)
    copies = []
    for i, cut in enumerate(blocks(width)):
        if cut.start < here:
            w = w_ref[:, cut]
        else:
            more[i - here // COLS].wait()
            w = wb_ref[:, cut.start - here : cut.stop - here]
        buf[:, cut] = (p_ref[:, cut] + dot(a_ref[...], w)).astype(BF16)
        wide = pl.ds(i * COLS, COLS)
        copies.append(pltpu.make_async_copy(buf.at[:, wide], out_hbm.at[:, wide], sems.at[i]))
        copies[-1].start()
    for copy in copies:
        copy.wait()


def out_last(a, w, partial, wb):
    rows, width = partial.shape
    depth = w.shape[0]
    return call(
        last_body,
        [("hbm", (rows, width), BF16)],
        [IN_VMEM] * 3 + [IN_HBM],
        (a, w, partial, wb),
        scratch=[
            pltpu.VMEM((depth, width - w.shape[1]), BF16),
            pltpu.VMEM((rows, width), BF16),
            pltpu.SemaphoreType.DMA((width // COLS,)),
            pltpu.SemaphoreType.DMA((width // COLS,)),
        ],
        limit=20,
        flops=2 * rows * depth * width,
    )


def swap(x):
    return lax.ppermute(x, "tp", [(0, 1), (1, 0)])


def scalar(x):
    return x.astype(jnp.int32).reshape(1)


def mixer(tokens, norm_gain, wq, wk, wv, wg, decay_bias, head_gain, wo):
    rows = tokens.shape[0]
    kw = wk.shape[1]
    heads = kw // HEAD_K
    tp = lax.axis_index("tp").astype(jnp.int32)
    start = (lax.axis_index(SP) * (2 * rows)).astype(jnp.int32)
    at, bt = scalar(start + tp * rows), scalar(start + (1 - tp) * rows)
    sequence = lax.axis_size(SP) * 2 * rows
    bias = decay_bias.astype(F32).reshape(1, kw)
    gain = norm_gain.astype(F32).reshape(1, -1)
    out_gain = head_gain.astype(F32).reshape(1, -1)
    far = functools.partial(pltpu.with_memory_space_constraint, memory_space=pltpu.HBM)

    late = scalar(lax.axis_index(OUTER))
    others = swap(tokens)
    xa, wk, wv, ka, va, sa = project_first(
        at, *map(far, (tokens, gain, bias, wk, wv)), sequence
    )
    xa, ka, va, xb, kb, vb, sb, state = project_second(
        bt, late, others, gain, bias, wk, wv, sa, xa, ka, va, sequence
    )
    other_wo = swap(wo)

    stretches = lax.axis_size(INNER)
    pieces = state.reshape(stretches, heads * HEAD_K // stretches, HEAD_V)
    got = lax.all_to_all(pieces, INNER, 0, 0, tiled=True)
    qa, qb, oa, ob = project_query(
        scalar(tp), at, bt, bias, sa, *map(far, (sb, ka, kb, va, vb, xa, xb, wq)), sequence
    )
    planes = lax.axis_size(("z1", "z0"))
    mirror = [(i, planes - 1 - i) for i in range(planes)]
    other_total = lax.ppermute(total_of(got), ("z1", "z0"), mirror)
    before = before_of(late, got, other_total)
    carried = lax.all_to_all(before, INNER, 0, 0, tiled=True)
    ga, gb = project_gate(out_gain, far(xa), far(xb), far(wg))
    carried = carried.reshape(heads, HEAD_K, HEAD_V)

    theirs = gate_theirs(late, qb, carried, ob, gb)
    received = swap(theirs)
    partial, wb = out_mine(late, qa, carried, oa, ga, far(wo), far(other_wo))
    return out_last(received, wb, partial, far(other_wo))


def solution(mesh):
    finer = Mesh(mesh.devices.reshape(2, 2, 4, 4, mesh.shape["tp"]), AXES)
    rows = P(AXES, None)
    cols = P(None, "tp")
    in_specs = (rows, P(), cols, cols, cols, cols, P("tp"), P("tp"), P("tp", None))
    return jax.shard_map(mixer, mesh=finer, in_specs=in_specs, out_specs=rows, check_vma=False)
```
